32 devices in a mesh: ep: 8 (over z, y), tp: 4 (over x, core).
Axes of the slice: x: 2, y: 2, z: 4, core: 2. Of those that a mesh axis runs over, the one named last changes fastest.
Arguments:
- tokens: bfloat16 [6144, 2048], P('ep')
- in_gain: float32 [2048], replicated, may hold values from 0.1 to 1.9
- route_ids: int32 [6144, 2], P('ep'), may hold values from 0 to 7, all different within a row; in each aligned block of 768 rows (0 to 767, 768 to 1535, ...) at most 384 rows name the same one
- route_scores: float32 [6144, 2], P('ep'), may hold values from 0.1 to 1
- gate_weight: bfloat16 [8, 2048, 1024], P('ep', None, 'tp'), may hold values from -0.125 to 0.125
- up_weight: bfloat16 [8, 2048, 1024], P('ep', None, 'tp'), may hold values from -0.125 to 0.125
- down_weight: bfloat16 [8, 1024, 2048], P('ep', 'tp')
- out_gain: float32 [2048], P('tp'), may hold values from 0.1 to 1.9
Outputs:
- mixed: bfloat16 [6144, 2048], P('ep', 'tp')
The draws below stay inside these ranges and needn't reach their ends.
Inputs may be any that keep to these rules, and one draw needn't show every extreme that they name: `route_ids`: each row names 2 different experts. Among the rows of one index of ep (aligned blocks of 768 rows) no expert is named more than 384 times, a bound that some block reaches.
All inputs are finite; a program needn't handle non-finite values.
Results may differ from the reference program's by a relative error of at most 0.012.
Values may be sent and summed in bfloat16 or wider, within the bound.
A program may use at most 128 MiB of HBM per device.

```python
import math
import jax
import jax.numpy as jnp
import numpy as np
from jax import lax

D = 2048
FF = 1024
TOP_K = 2
TOK_DEV = 768
EXPERTS = 8
TOKENS = 6144
CAP = 384
FF_PART = 256
N_EP = 8
N_TP = 4


def draw_tokens(key, part):
    keys = jax.random.split(jax.random.fold_in(key, 3), 3)
    row_scale = 10.0 ** jax.random.uniform(keys[1], (TOKENS, 1), jnp.float32)
    column_scale = 10.0 ** (0.5 * jax.random.uniform(keys[2], (1, D), jnp.float32))
    values = jax.random.normal(keys[0], (TOKENS, D), jnp.float32) * row_scale * column_scale
    return values.astype(jnp.bfloat16)


def draw_down_weight(key, part):
    keys = jax.random.split(jax.random.fold_in(key, 11), 2)
    position = jnp.arange(D, dtype=jnp.float32) / D
    base = jax.random.normal(keys[0], (EXPERTS, FF, D), jnp.float32)
    scale = 10.0 ** (0.5 * position + 0.5 * jax.random.uniform(keys[1], (D,), jnp.float32))
    return (base * FF ** (-0.5) * scale[None, None, :]).astype(jnp.bfloat16)


def steps_of(stream_key, dims, pieces, smallest, top_value):
    loudness = 1.0
    for dim, parts in pieces:
        draws = jax.random.uniform(jax.random.fold_in(jax.random.fold_in(stream_key, 6), dim), (parts,), jnp.float32, smallest / len(pieces), top_value / len(pieces))
        loudness = loudness * jnp.repeat(jnp.exp(draws), dims[dim] // parts).reshape((-1,) + (1,) * (len(dims) - 1 - dim))
    return loudness


def routed_block(own_key, own, number, rows, count, top, reach, lean):
    sequence = jax.random.permutation(own_key, count)
    crowded, usual = shares(count, rows * top, reach, lean, True), shares(count, rows * top, reach, lean, False)
    places = jnp.arange(count)

    def named(tallies, rotation):
        used = int((tallies > 0).sum())
        fixed = max(1, used // 4)
        moved = fixed + (places - fixed + rotation * (used - fixed)) % max(1, count - fixed)
        return jnp.zeros((count,), jnp.int32).at[sequence[jnp.where(places < fixed, places, moved)]].set(jnp.asarray(tallies, jnp.int32))

    tallies = jnp.where(number % 4 == 0, named(crowded, number // 4), named(usual, number - number // 4 - 1))
    mixed = jax.random.permutation(jax.random.fold_in(own, 3), count)
    giver, sink = mixed[0:count // 2 * 2:2], mixed[1:count // 2 * 2:2]
    margin = jnp.minimum(tallies[giver] - 1, reach - tallies[sink]) // 2
    margin = jnp.where((giver == sequence[0]) | (sink == sequence[0]) | (tallies[sink] == 0), 0, jnp.maximum(margin, 0))
    moved = jax.random.randint(jax.random.fold_in(own, 4), (count // 2,), 0, 1 << 20) % (margin + 1)
    tallies = tallies.at[giver].add(-moved).at[sink].add(moved)
    labels = jnp.searchsorted(jnp.cumsum(tallies), jnp.arange(rows * top), side="right").astype(jnp.int32)
    listing = labels.reshape(top, rows).T
    listing = listing[jax.random.permutation(jax.random.fold_in(own, 1), rows)]
    rotation = jax.random.randint(jax.random.fold_in(own, 2), (rows, 1), 0, top)
    return jnp.take_along_axis(listing, (jnp.arange(top)[None, :] + rotation) % top, axis=1)


def shares(count, total, most, slope, full):
    weights = [(1 << 20) // math.isqrt(standing ** slope) + 1 for standing in range(1, count + 1)]
    largest = most if full else min(most, max(-(-total // count), total * weights[0] // sum(weights)))
    least = 1 if total - largest >= count - 1 else 0
    counts, spare = [largest] + [least] * (count - 1), total - largest - least * (count - 1)
    while spare > 0:
        candidates = [i for i in range(1, count) if counts[i] < largest] or [i for i in range(1, count) if counts[i] < most]
        pool, left = sum([weights[i] for i in candidates]), spare
        for i in candidates:
            addition = min(most - counts[i], max(1, left * weights[i] // pool), spare)
            counts[i] = counts[i] + addition
            spare = spare - addition
    return np.array(counts)


def noise(stream_key, shape, scale, most, cuts=(), kind=jnp.bfloat16):
    values = scale * jax.random.normal(stream_key, shape, jnp.float32)
    if cuts:
        values = values * steps_of(stream_key, shape, cuts, -0.22, 0.18)
    return jnp.clip(values, -most, most).astype(kind)


def setup_inputs(seed: int = 0) -> dict:
    key_of = jax.random.split(jax.random.key(seed), 9)
    tokens = draw_tokens(jax.random.fold_in(key_of[8], 71), 0)
    in_gain = jnp.clip(1.0 + 0.18 * jax.random.normal(key_of[1], (D,), jnp.float32), 0.1, 1.9)
    route_ids_keys = jax.random.split(jax.random.fold_in(key_of[2], 1), TOKENS // TOK_DEV)
    route_ids_turns = jax.random.permutation(jax.random.fold_in(key_of[2], 3), TOKENS // TOK_DEV)
    route_ids = jax.vmap(lambda own, number: routed_block(jax.random.fold_in(key_of[2], 2), own, number, TOK_DEV, EXPERTS, TOP_K, CAP, 2))(route_ids_keys, route_ids_turns).reshape((TOKENS, TOP_K))
    route_scores = jnp.clip(jnp.exp(math.log(1.0) - 2.3025851 * jax.random.uniform(key_of[3], (TOKENS, TOP_K), jnp.float32) ** steps_of(key_of[3], (TOKENS, TOP_K), ((0, 8),), -0.2, 0.2)), 0.1, 1.0)
    gate_weight = noise(key_of[4], (EXPERTS, D, FF), D ** -0.5, 0.125, ((0, 8), (2, 4)))
    up_weight = noise(key_of[5], (EXPERTS, D, FF), D ** -0.5, 0.125, ((0, 8), (2, 4)))
    down_weight = draw_down_weight(jax.random.fold_in(key_of[8], 71), 0)
    out_gain = jnp.clip(1.0 + 0.18 * jax.random.normal(key_of[7], (D,), jnp.float32), 0.1, 1.9)
    return dict(tokens=tokens, in_gain=in_gain, route_ids=route_ids, route_scores=route_scores, gate_weight=gate_weight, up_weight=up_weight, down_weight=down_weight, out_gain=out_gain)


epsilon = 1e-06

def reference(tokens, in_gain, route_ids, route_scores, gate_weight, up_weight, down_weight, out_gain):
    as_float = tokens.astype(jnp.float32)
    normed = (as_float * lax.rsqrt(lax.optimization_barrier(jnp.mean(as_float * as_float, axis=1, keepdims=True)) + epsilon) * in_gain).astype(jnp.bfloat16)
    flat_ids = route_ids.reshape(N_EP, TOK_DEV * TOP_K)
    one_hot = (flat_ids[:, :, None] == jnp.arange(EXPERTS, dtype=jnp.int32)[None, None, :]).astype(jnp.int32)
    slot_index = lax.optimization_barrier(jnp.sum((jnp.cumsum(one_hot, axis=1) - 1) * one_hot, axis=2)).astype(jnp.int32)
    block_index = jnp.broadcast_to(jnp.arange(N_EP, dtype=jnp.int32)[:, None], flat_ids.shape)
    row_index = (block_index * TOK_DEV + jnp.arange(TOK_DEV * TOP_K, dtype=jnp.int32)[None, :] // TOP_K).astype(jnp.int32)
    buffer = jnp.zeros((EXPERTS, N_EP, CAP, D), jnp.bfloat16)
    buffer = buffer.at[flat_ids, block_index, slot_index].set(normed[row_index])

    def expert_run(inputs):
        rows_in, gate_w, up_w, down_w = inputs
        gate_acts = jnp.dot(rows_in, gate_w, preferred_element_type=jnp.float32)
        up_acts = jnp.dot(rows_in, up_w, preferred_element_type=jnp.float32)
        hidden = (jax.nn.silu(gate_acts) * up_acts).astype(jnp.bfloat16)
        hidden_blocks = hidden.reshape(-1, N_TP, FF_PART).astype(jnp.float32)
        down_blocks = down_w.reshape(N_TP, FF_PART, D).astype(jnp.float32)
        partial_value = jnp.einsum('rpf,pfd->prd', hidden_blocks, down_blocks)
        rounded = lax.optimization_barrier(partial_value.astype(jnp.bfloat16))
        return lax.optimization_barrier(jnp.sum(rounded.astype(jnp.float32), axis=0)).astype(jnp.bfloat16)
    outputs = lax.map(expert_run, (buffer.reshape(EXPERTS, N_EP * CAP, D), gate_weight, up_weight, down_weight))
    outputs = outputs.reshape(EXPERTS, N_EP, CAP, D)
    picked = outputs[flat_ids, block_index, slot_index].astype(jnp.float32).reshape(TOKENS, TOP_K, D)
    mix_weight = route_scores / lax.optimization_barrier(jnp.sum(route_scores, axis=1, keepdims=True))
    combined = lax.optimization_barrier(jnp.sum(mix_weight[:, :, None] * picked, axis=1))
    mixed = combined * lax.rsqrt(lax.optimization_barrier(jnp.mean(combined * combined, axis=1, keepdims=True)) + epsilon) * out_gain
    return mixed.astype(jnp.bfloat16)
```

```python
import functools

import jax
import jax.numpy as jnp
from jax import lax
from jax.experimental import pallas as pl
from jax.experimental.pallas import tpu as pltpu
from jax.sharding import PartitionSpec as P

epsilon = 1e-06
MESH = pl.DeviceIdType.MESH


def gathered(block, count):
    blocks = [block]
    bit = 1
    swaps = []
    while bit < count:
        swaps.append([(i, i ^ bit) for i in range(count)])
        bit *= 2
    first = lax.ppermute(block, "tp", swaps[0])
    blocks.append(first)
    for pairs in swaps[1:]:
        far = lax.ppermute(block, "tp", pairs)
        blocks.append(far)
        blocks.append(lax.ppermute(far, "tp", swaps[0]))
    return blocks


def per_device(
    tokens, in_gain, route_ids, route_scores, gate_weight, up_weight, down_weight, out_gain
):
    count_ep = lax.axis_size("ep")
    count_tp = lax.axis_size("tp")
    experts = count_ep * gate_weight.shape[0]
    tok_count, full_width = tokens.shape
    rows = tok_count // count_tp
    start = lax.axis_index("tp") * rows
    gates = gathered(gate_weight[0], count_tp)
    ups = gathered(up_weight[0], count_tp)
    downs = gathered(down_weight[0], count_tp)
    gain_full = lax.all_gather(out_gain, "tp", axis=0, tiled=True)

    as_float = lax.dynamic_slice_in_dim(tokens, start, rows, 0).astype(jnp.float32)
    normed = (
        as_float
        * lax.rsqrt(jnp.mean(as_float * as_float, axis=1, keepdims=True) + epsilon)
        * in_gain
    ).astype(jnp.bfloat16)
    ring = count_ep // 2
    pair_swap = [(i, i ^ 1) for i in range(count_ep)]
    ring_step = [(i, (i + 2) % count_ep) for i in range(count_ep)]
    held = [normed]
    for _ in range(1, ring):
        held.append(lax.ppermute(held[-1], "ep", ring_step))
    partner = [lax.ppermute(block, "ep", pair_swap) for block in held]

    ids = lax.dynamic_slice_in_dim(route_ids, start, rows, 0)
    scores = lax.dynamic_slice_in_dim(route_scores, start, rows, 0)
    mix = scores / jnp.sum(scores, axis=1, keepdims=True)
    chosen = ids[:, :, None] == jnp.arange(experts, dtype=jnp.int32)[None, None, :]
    dense = jnp.sum(jnp.where(chosen, mix[:, :, None], 0.0), axis=1).T
    weight = lax.all_to_all(dense, "ep", split_axis=0, concat_axis=0, tiled=True).reshape(count_ep, rows)

    gates, ups, held = lax.optimization_barrier((gates, ups, held))
    gate_full = jnp.concatenate(gates, 1)
    up_full = jnp.concatenate(ups, 1)
    down_full = jnp.concatenate(downs, 0)
    me = lax.axis_index("ep")

    def terms_of(step):
        block = jnp.concatenate([held[step], partner[step]], 0)
        gate_acts = jnp.dot(block, gate_full, preferred_element_type=jnp.float32)
        up_acts = jnp.dot(block, up_full, preferred_element_type=jnp.float32)
        hidden = (jax.nn.silu(gate_acts) * up_acts).astype(jnp.bfloat16)
        expert_out = jnp.dot(hidden, down_full, preferred_element_type=jnp.float32)
        source = (me + count_ep - 2 * step) % count_ep
        share = jnp.concatenate(
            [
                lax.dynamic_index_in_dim(weight, source, 0, keepdims=False),
                lax.dynamic_index_in_dim(weight, source ^ 1, 0, keepdims=False),
            ]
        )[:, None]
        terms = jnp.where(share > 0.0, share * expert_out, 0.0).astype(jnp.bfloat16)
        return terms[:rows], terms[rows:]

    running = None
    for step in list(range(1, ring)) + [0]:
        own, other = terms_of(step)
        total = own.astype(jnp.float32) + lax.ppermute(other, "ep", pair_swap).astype(jnp.float32)
        if running is not None:
            total = total + lax.ppermute(running, "ep", ring_step).astype(jnp.float32)
        running = total.astype(jnp.bfloat16)
    combined = total
    scale = lax.rsqrt(jnp.mean(combined * combined, axis=1, keepdims=True) + epsilon)
    mixed = (combined * scale * gain_full).astype(jnp.bfloat16)
    return lax.all_to_all(mixed, "tp", split_axis=1, concat_axis=0, tiled=True)


END, MID = 0, 1
INW, OUTW, PAIR = 0, 1, 2
LINE = 4
QUARTERS = 4
SLOTS = 14


def send_tables():
    sends = {(k, l): {} for k in (END, MID) for l in (INW, OUTW, PAIR)}
    for q in range(QUARTERS):
        sends[END, INW][q] = ("O", 0, q)
        sends[END, INW][4 + q] = ("P", 0, q)
        sends[END, PAIR][q] = ("O", 0, q)
        sends[END, PAIR][6 + q] = ("O", 2, q)
        sends[END, PAIR][10 + q] = ("O", 3, q)
        sends[MID, OUTW][q] = ("O", 1, q)
        sends[MID, OUTW][4 + q] = ("O", 2, q)
        sends[MID, OUTW][8 + q] = ("O", 3, q)
        sends[MID, INW][q] = ("O", 1, q)
        sends[MID, INW][4 + q] = ("O", 0, q)
        for b in (1, 2, 3):
            sends[MID, PAIR][4 * (b - 1) + q] = ("O", b, q)
    for q in (0, 1):
        sends[END, PAIR][4 + q] = ("O", 1, q)
        sends[MID, OUTW][12 + q] = ("P", 1, 2 + q)
    other = {"O": "P", "P": "O"}
    cross = lambda p: (other[p[0]], p[1], p[2])
    mirror = lambda p: (p[0], LINE - 1 - p[1], p[2])
    recvs = {
        (END, INW): dict(sends[MID, OUTW]),
        (END, OUTW): {},
        (END, PAIR): {s: cross(p) for s, p in sends[END, PAIR].items()},
        (MID, INW): {s: mirror(p) for s, p in sends[MID, INW].items()},
        (MID, OUTW): dict(sends[END, INW]),
        (MID, PAIR): {s: cross(p) for s, p in sends[MID, PAIR].items()},
    }
    return sends, recvs


SENDS, RECVS = send_tables()
ORDER = {
    END: [("O", 0), ("P", 0), ("O", 1), ("O", 2), ("P", 2), ("O", 3), ("P", 3), ("P", 1)],
    MID: [("O", 1), ("O", 0), ("O", 2), ("P", 1), ("P", 0), ("O", 3), ("P", 2), ("P", 3)],
}


def children(kind, piece):
    return [(l, s) for l in (INW, OUTW, PAIR) for s, p in SENDS[kind, l].items() if p == piece]


def fused_kernel(
    tok_ref, gain_ref, dense_ref, gate_ref, up_ref, down_ref, out_ref,
    tok_buf, xs, wg, wu, wd, hid, res, rin, rout, fin, wts, wcol,
    local_sem, w_send, w_recv, m_send, m_recv, d_send, d_recv, r_send, r_recv, f_send, f_recv,
):
    me, tp = lax.axis_index("ep"), lax.axis_index("tp")
    count_ep, rows, width = xs.shape
    count_tp = wg.shape[0]
    part = wg.shape[2]
    piece_rows = rows // QUARTERS
    none = rin.shape[0] - 1
    z, y = me // 2, me % 2
    low = z < LINE // 2
    is_end = (z == 0) | (z == LINE - 1)
    is_mid = jnp.logical_not(is_end)
    pick = lambda a, b: jnp.where(is_end, a, b)
    inward = jnp.where(low, z + 1, z - 1) * 2 + y
    outward = jnp.where(low, z - 1, z + 1) * 2 + y
    pair = z * 2 + 1 - y
    links = (inward, outward, pair)
    far_link = (pick(OUTW, INW), INW, PAIR)

    def block_of(column, b):
        line = jnp.where(low, b, LINE - 1 - b)
        return line * 2 + (y if column == "O" else 1 - y)

    def for_kinds(table, body):
        if END in table and MID in table:
            body(table[END], table[MID])
        elif END in table:
            pl.when(is_end)(lambda: body(table[END], table[END]))
        elif MID in table:
            pl.when(is_mid)(lambda: body(table[MID], table[MID]))

    def place(a, b):
        block = pick(block_of(a[0], a[1]), block_of(b[0], b[1]))
        return block, pick(a[2], b[2]) if a[2] != b[2] else a[2]

    def at(table, link, s):
        return {k: table[k, link][s] for k in (END, MID) if s in table[k, link]}

    own_rows = pltpu.make_async_copy(tok_ref.at[pl.ds(tp * rows, rows)], tok_buf, local_sem.at[0])
    own_rows.start()
    mine = [
        pltpu.make_async_copy(src, dst.at[tp], local_sem.at[1 + i])
        for i, (src, dst) in enumerate(((gate_ref, wg), (up_ref, wu), (down_ref, wd)))
    ]
    for copy in mine:
        copy.start()

    barrier = pltpu.get_barrier_semaphore()
    for step in range(1, count_ep):
        pl.semaphore_signal(barrier, inc=1, device_id=(lax.rem(me + step, count_ep), tp), device_id_type=MESH)
    for step in range(1, count_tp):
        pl.semaphore_signal(barrier, inc=1, device_id=(me, lax.rem(tp + step, count_tp)), device_id_type=MESH)

    own_rows.wait()
    group = 16

    def norm(i, carry):
        at_rows = pl.ds(pl.multiple_of(i * group, group), group)
        value = tok_buf[at_rows, :].astype(jnp.float32)
        scale = lax.rsqrt(jnp.mean(value * value, axis=1, keepdims=True) + epsilon)
        xs[me, at_rows, :] = (value * scale * gain_ref[...]).astype(jnp.bfloat16)
        return carry

    lax.fori_loop(0, rows // group, norm, 0)
    rin[none] = jnp.zeros(rin.shape[1:], rin.dtype)
    pl.semaphore_wait(barrier, count_ep + count_tp - 2)

    near, far = tp + 1 - 2 * (tp % 2), lax.rem(tp + 2, count_tp)
    diagonal = far + 1 - 2 * (far % 2)
    trio = ((gate_ref, wg), (up_ref, wu), (down_ref, wd))

    def weight_copy(i, kind, src, dst, target):
        return pltpu.make_async_remote_copy(
            src_ref=src, dst_ref=dst, send_sem=w_send.at[kind, i], recv_sem=w_recv.at[kind, i],
            device_id=(me, target), device_id_type=MESH,
        )

    over_x = [weight_copy(i, 0, s, d.at[tp], far) for i, (s, d) in enumerate(trio)]
    to_near = [weight_copy(i, 1, s, d.at[tp], near) for i, (s, d) in enumerate(trio)]
    onward = [weight_copy(i, 2, d.at[far], d.at[far], near) for i, (s, d) in enumerate(trio)]
    in_x = [weight_copy(i, 0, d.at[far], d.at[far], far) for i, (s, d) in enumerate(trio)]
    in_near = [weight_copy(i, 1, d.at[near], d.at[near], near) for i, (s, d) in enumerate(trio)]
    in_onward = [weight_copy(i, 2, d.at[diagonal], d.at[diagonal], near) for i, (s, d) in enumerate(trio)]

    def mix_copy(step):
        target = lax.rem(me + step, count_ep)
        return pltpu.make_async_remote_copy(
            src_ref=dense_ref, dst_ref=wts.at[me], send_sem=m_send.at[step - 1], recv_sem=m_recv.at[step - 1],
            device_id=(target, tp), device_id_type=MESH,
        )

    def mix_wait(step):
        source = lax.rem(me + count_ep - step, count_ep)
        pltpu.make_async_remote_copy(
            src_ref=dense_ref, dst_ref=wts.at[source], send_sem=m_send.at[step - 1], recv_sem=m_recv.at[step - 1],
            device_id=(source, tp), device_id_type=MESH,
        ).wait_recv()

    def row_copy(link, s, piece):
        block, q = piece
        ref = xs.at[block, pl.ds(q * piece_rows, piece_rows)]
        return pltpu.make_async_remote_copy(
            src_ref=ref, dst_ref=ref, send_sem=d_send.at[link, s], recv_sem=d_recv.at[far_link[link], s],
            device_id=(links[link], tp), device_id_type=MESH,
        )

    def row_arrival(link, s, piece):
        block, q = piece
        ref = xs.at[block, pl.ds(q * piece_rows, piece_rows)]
        return pltpu.make_async_remote_copy(
            src_ref=ref, dst_ref=ref, send_sem=d_send.at[link, s], recv_sem=d_recv.at[link, s],
            device_id=(links[link], tp), device_id_type=MESH,
        )

    order = [pick(block_of(*ORDER[END][k]), block_of(*ORDER[MID][k])) for k in range(count_ep)]

    def ordered(k):
        block = order[0]
        for i in range(1, count_ep):
            block = jnp.where(k == i, order[i], block)
        return block

    def gate_up(first, last, sources):
        def body(i, carry):
            block = ordered(first + i // len(sources))
            source = sources[0]
            for n in range(1, len(sources)):
                source = jnp.where(i % len(sources) == n, sources[n], source)
            x = xs[block]
            gate = jnp.dot(x, wg[source], preferred_element_type=jnp.float32)
            up = jnp.dot(x, wu[source], preferred_element_type=jnp.float32)
            hidden = gate / (1.0 + jnp.exp(-gate)) * up
            hid[block, :, pl.ds(pl.multiple_of(source * part, part), part)] = hidden.astype(jnp.bfloat16)
            return carry

        lax.fori_loop(0, (last - first) * len(sources), body, 0)

    tiles = width // part

    def down(first, last):
        def body(i, carry):
            block = ordered(first + i // tiles)
            columns = pl.ds(pl.multiple_of((i % tiles) * part, part), part)
            value = jnp.zeros((rows, part), jnp.float32)
            for j in range(count_tp):
                value = value + jnp.dot(
                    hid[block, :, j * part:(j + 1) * part], wd[j, :, columns], preferred_element_type=jnp.float32
                )
            share = wcol[block][:, :1]
            res[block, :, columns] = jnp.where(share > 0.0, share * value, 0.0).astype(jnp.bfloat16)
            return carry

        lax.fori_loop(0, (last - first) * tiles, body, 0)

    def dispatch_sends(s):
        for link in (INW, OUTW, PAIR):
            for_kinds(at(SENDS, link, s), lambda a, b: row_copy(link, s, place(a, b)).start())

    def dispatch_waits(s):
        for link in (INW, OUTW, PAIR):
            for_kinds(at(RECVS, link, s), lambda a, b: row_arrival(link, s, place(a, b)).wait_recv())

    for s in range(SLOTS):
        if s >= 2:
            dispatch_waits(s - 2)
        dispatch_sends(s)
        if s == 0:
            for copy in over_x:
                copy.start()
            for copy in to_near:
                copy.start()
        if s == 1:
            wts[me] = dense_ref[...]
            for step in range(1, count_ep):
                mix_copy(step).start()
            for copy in mine:
                copy.wait()
            for copy in in_near:
                copy.wait_recv()
            gate_up(0, 1, (tp, near))
        if s == 5:
            gate_up(1, 2, (tp, near))
        if s == 6:
            gate_up(2, 3, (tp, near))
        if s == 7:
            in_x[0].wait_recv()
            onward[0].start()
            for step in range(1, count_ep):
                mix_wait(step)
            for block in range(count_ep):
                turned = jnp.transpose(wts[block])
                lane = lax.broadcasted_iota(jnp.int32, turned.shape, 1)
                column = jnp.sum(jnp.where(lane == me, turned, 0.0), axis=1, keepdims=True)
                wcol[block] = jnp.broadcast_to(column[:rows], (rows, 128))
        if s == 9:
            gate_up(3, 4, (tp, near))
        if s == 11:
            gate_up(4, 5, (tp, near))
        if s == 12:
            in_x[1].wait_recv()
            onward[1].start()
        if s == 13:
            gate_up(5, 6, (tp, near))
            in_onward[0].wait_recv()
            in_onward[1].wait_recv()
            gate_up(0, 4, (far, diagonal))
    dispatch_waits(SLOTS - 2)
    dispatch_waits(SLOTS - 1)
    gate_up(4, 6, (far, diagonal))
    gate_up(6, 8, (tp, near, far, diagonal))
    in_x[2].wait_recv()
    onward[2].start()
    in_onward[2].wait_recv()
    down(0, 8)

    def back_copy(link, s):
        return pltpu.make_async_remote_copy(
            src_ref=rout.at[link * SLOTS + s], dst_ref=rin.at[far_link[link] * SLOTS + s],
            send_sem=r_send.at[link, s], recv_sem=r_recv.at[far_link[link], s],
            device_id=(links[link], tp), device_id_type=MESH,
        )

    def back_wait(link, s):
        pltpu.make_async_remote_copy(
            src_ref=rout.at[link * SLOTS + s], dst_ref=rin.at[link * SLOTS + s],
            send_sem=r_send.at[link, s], recv_sem=r_recv.at[link, s],
            device_id=(links[link], tp), device_id_type=MESH,
        ).wait_recv()

    def wait_children(pieces):
        kids = {k: children(k, p) for k, p in pieces.items()}
        shared = [c for c in kids.get(END, []) if c in kids.get(MID, [])]
        for c in shared:
            back_wait(*c)
        for kind, cond in ((END, is_end), (MID, is_mid)):
            extra = [c for c in kids.get(kind, []) if c not in shared]
            if extra and len(kids) == 1:
                for c in extra:
                    back_wait(*c)
            elif extra:
                def waits(extra=extra):
                    for c in extra:
                        back_wait(*c)
                pl.when(cond)(waits)
        return kids

    def slot_of(child):
        return child[0] * SLOTS + child[1]

    def child_index(kids, n):
        ids = {k: slot_of(v[n]) if n < len(v) else none for k, v in kids.items()}
        if len(ids) == 1:
            return next(iter(ids.values()))
        return pick(ids[END], ids[MID]) if ids[END] != ids[MID] else ids[END]

    def back_slot(link, s):
        def body(pieces):
            kids = wait_children(pieces)
            most = max(len(v) for v in kids.values())
            values = list(pieces.values())
            block, q = place(values[0], values[-1])
            first = q * piece_rows
            total_rows = pl.ds(first, piece_rows)
            sources = [child_index(kids, n) for n in range(most)]

            def add(i, carry):
                at_rows = pl.ds(pl.multiple_of(i * group, group), group)
                from_rows = pl.ds(pl.multiple_of(first + i * group, group), group)
                total = res[block, from_rows, :].astype(jnp.float32)
                for source in sources:
                    total = total + rin[source, at_rows, :].astype(jnp.float32)
                rout[link * SLOTS + s, at_rows, :] = total.astype(jnp.bfloat16)
                return carry

            lax.fori_loop(0, piece_rows // group, add, 0)
            back_copy(link, s).start()

        table = at(RECVS, link, s)
        if END in table and MID in table:
            body(table)
        elif END in table:
            pl.when(is_end)(lambda: body(table))
        elif MID in table:
            pl.when(is_mid)(lambda: body(table))

    def final_copy(q, step):
        target = lax.rem(tp + step, count_tp)
        rows_at = pl.ds(q * piece_rows, piece_rows)
        return pltpu.make_async_remote_copy(
            src_ref=fin.at[target, rows_at], dst_ref=out_ref.at[tp, rows_at],
            send_sem=f_send.at[q, step - 1], recv_sem=f_recv.at[q, step - 1],
            device_id=(me, target), device_id_type=MESH,
        )

    def final_wait(q, step):
        source = lax.rem(tp + count_tp - step, count_tp)
        rows_at = pl.ds(q * piece_rows, piece_rows)
        pltpu.make_async_remote_copy(
            src_ref=fin.at[source, rows_at], dst_ref=out_ref.at[source, rows_at],
            send_sem=f_send.at[q, step - 1], recv_sem=f_recv.at[q, step - 1],
            device_id=(me, source), device_id_type=MESH,
        ).wait_recv()

    def finish(q):
        pieces = {END: ("O", 0, q), MID: ("O", 1, q)}
        kids = wait_children(pieces)
        sources = [child_index(kids, n) for n in range(3)]
        columns = width // count_tp

        def body(i, carry):
            at_rows = pl.ds(pl.multiple_of(i * group, group), group)
            own = pl.ds(pl.multiple_of(q * piece_rows + i * group, group), group)
            total = res[me, own, :].astype(jnp.float32)
            for source in sources:
                total = total + rin[source, at_rows, :].astype(jnp.float32)
            scale = lax.rsqrt(jnp.mean(total * total, axis=1, keepdims=True) + epsilon)
            mixed = (total * scale).astype(jnp.bfloat16)
            for c in range(count_tp):
                fin[c, own, :] = mixed[:, c * columns:(c + 1) * columns]
            return carry

        lax.fori_loop(0, piece_rows // group, body, 0)
        for step in range(1, count_tp):
            final_copy(q, step).start()

    for r in range(SLOTS):
        s = SLOTS - 1 - r
        for link in (PAIR, INW, OUTW):
            back_slot(link, s)
        if s + 2 < QUARTERS:
            finish(s + 2)
    finish(1)
    finish(0)
    keep = pltpu.make_async_copy(fin.at[tp], out_ref.at[tp], local_sem.at[0])
    keep.start()

    for link in (INW, OUTW, PAIR):
        for s in range(SLOTS):
            for_kinds(at(SENDS, link, s), lambda a, b: row_copy(link, s, place(a, b)).wait_send())
            for_kinds(at(RECVS, link, s), lambda a, b: back_copy(link, s).wait_send())
    for copies in (over_x, to_near, onward):
        for copy in copies:
            copy.wait_send()
    for step in range(1, count_ep):
        mix_copy(step).wait_send()
    for q in range(QUARTERS):
        for step in range(1, count_tp):
            final_copy(q, step).wait_send()
            final_wait(q, step)
    keep.wait()


def fused(tokens, in_gain, route_ids, route_scores, gate_weight, up_weight, down_weight, out_gain):
    count_ep, count_tp = lax.axis_size("ep"), lax.axis_size("tp")
    experts = count_ep * gate_weight.shape[0]
    tok_count, width = tokens.shape
    rows = tok_count // count_tp
    part = gate_weight.shape[2]
    start = lax.axis_index("tp") * rows
    ids = lax.dynamic_slice_in_dim(route_ids, start, rows, 0)
    scores = lax.dynamic_slice_in_dim(route_scores, start, rows, 0)
    mix = scores / jnp.sum(scores, axis=1, keepdims=True)
    chosen = ids[:, :, None] == jnp.arange(experts, dtype=jnp.int32)[None, None, :]
    dense = jnp.sum(jnp.where(chosen, mix[:, :, None], 0.0), axis=1).T
    lanes = -(-rows // 128) * 128
    dense = jnp.pad(dense, ((0, 0), (0, lanes - rows)))
    piece = (rows // QUARTERS, width)
    bf16, f32 = jnp.bfloat16, jnp.float32
    dma = pltpu.SemaphoreType.DMA
    any_space = pl.BlockSpec(memory_space=pltpu.HBM)
    in_vmem = pl.BlockSpec(memory_space=pltpu.VMEM)
    out = pl.pallas_call(
        fused_kernel,
        name="experts",
        out_shape=jax.ShapeDtypeStruct((count_tp, rows, width // count_tp), bf16),
        in_specs=[any_space, in_vmem, in_vmem, any_space, any_space, any_space],
        out_specs=any_space,
        scratch_shapes=[
            pltpu.VMEM((rows, width), bf16),
            pltpu.VMEM((count_ep, rows, width), bf16),
            pltpu.VMEM((count_tp, width, part), bf16),
            pltpu.VMEM((count_tp, width, part), bf16),
            pltpu.VMEM((count_tp, part, width), bf16),
            pltpu.VMEM((count_ep, rows, part * count_tp), bf16),
            pltpu.VMEM((count_ep, rows, width), bf16),
            pltpu.VMEM((3 * SLOTS + 1,) + piece, bf16),
            pltpu.VMEM((3 * SLOTS,) + piece, bf16),
            pltpu.VMEM((count_tp, rows, width // count_tp), bf16),
            pltpu.VMEM((count_ep, experts, lanes), f32),
            pltpu.VMEM((count_ep, rows, 128), f32),
            dma((4,)),
            dma((3, 3)),
            dma((3, 3)),
            dma((count_ep - 1,)),
            dma((count_ep - 1,)),
            dma((3, SLOTS)),
            dma((3, SLOTS)),
            dma((3, SLOTS)),
            dma((3, SLOTS)),
            dma((QUARTERS, count_tp - 1)),
            dma((QUARTERS, count_tp - 1)),
        ],
        compiler_params=pltpu.CompilerParams(
            collective_id=0, has_side_effects=True, vmem_limit_bytes=63 * 2**20
        ),
    )(tokens, in_gain.reshape(1, width), dense, gate_weight[0], up_weight[0], down_weight[0])
    out = out.reshape(tok_count, width // count_tp)
    return (out.astype(f32) * out_gain).astype(bf16)


def solution(mesh):
    in_specs = (
        P("ep", None),
        P(),
        P("ep", None),
        P("ep", None),
        P("ep", None, "tp"),
        P("ep", None, "tp"),
        P("ep", "tp", None),
        P("tp"),
    )
    out_specs = P("ep", "tp")
    small = mesh.shape["ep"] == 2 * LINE and mesh.shape["tp"] == QUARTERS
    return jax.shard_map(
        fused if small else per_device, mesh=mesh, in_specs=in_specs, out_specs=out_specs, check_vma=False
    )
```

```python
import functools

import jax
import jax.numpy as jnp
from jax import lax
from jax.experimental import pallas as pl
from jax.experimental.pallas import tpu as pltpu
from jax.sharding import PartitionSpec as P

epsilon = 1e-06
MESH = pl.DeviceIdType.MESH


def gathered(block, count):
    blocks = [block]
    bit = 1
    swaps = []
    while bit < count:
        swaps.append([(i, i ^ bit) for i in range(count)])
        bit *= 2
    first = lax.ppermute(block, "tp", swaps[0])
    blocks.append(first)
    for pairs in swaps[1:]:
        far = lax.ppermute(block, "tp", pairs)
        blocks.append(far)
        blocks.append(lax.ppermute(far, "tp", swaps[0]))
    return blocks


def per_device(
    tokens, in_gain, route_ids, route_scores, gate_weight, up_weight, down_weight, out_gain
):
    count_ep = lax.axis_size("ep")
    count_tp = lax.axis_size("tp")
    experts = count_ep * gate_weight.shape[0]
    tok_count, full_width = tokens.shape
    rows = tok_count // count_tp
    start = lax.axis_index("tp") * rows
    gates = gathered(gate_weight[0], count_tp)
    ups = gathered(up_weight[0], count_tp)
    downs = gathered(down_weight[0], count_tp)
    gain_full = lax.all_gather(out_gain, "tp", axis=0, tiled=True)

    as_float = lax.dynamic_slice_in_dim(tokens, start, rows, 0).astype(jnp.float32)
    normed = (
        as_float
        * lax.rsqrt(jnp.mean(as_float * as_float, axis=1, keepdims=True) + epsilon)
        * in_gain
    ).astype(jnp.bfloat16)
    ring = count_ep // 2
    pair_swap = [(i, i ^ 1) for i in range(count_ep)]
    ring_step = [(i, (i + 2) % count_ep) for i in range(count_ep)]
    held = [normed]
    for _ in range(1, ring):
        held.append(lax.ppermute(held[-1], "ep", ring_step))
    partner = [lax.ppermute(block, "ep", pair_swap) for block in held]

    ids = lax.dynamic_slice_in_dim(route_ids, start, rows, 0)
    scores = lax.dynamic_slice_in_dim(route_scores, start, rows, 0)
    mix = scores / jnp.sum(scores, axis=1, keepdims=True)
    chosen = ids[:, :, None] == jnp.arange(experts, dtype=jnp.int32)[None, None, :]
    dense = jnp.sum(jnp.where(chosen, mix[:, :, None], 0.0), axis=1).T
    weight = lax.all_to_all(dense, "ep", split_axis=0, concat_axis=0, tiled=True).reshape(count_ep, rows)

    gates, ups, held = lax.optimization_barrier((gates, ups, held))
    gate_full = jnp.concatenate(gates, 1)
    up_full = jnp.concatenate(ups, 1)
    down_full = jnp.concatenate(downs, 0)
    me = lax.axis_index("ep")

    def terms_of(step):
        block = jnp.concatenate([held[step], partner[step]], 0)
        gate_acts = jnp.dot(block, gate_full, preferred_element_type=jnp.float32)
        up_acts = jnp.dot(block, up_full, preferred_element_type=jnp.float32)
        hidden = (jax.nn.silu(gate_acts) * up_acts).astype(jnp.bfloat16)
        expert_out = jnp.dot(hidden, down_full, preferred_element_type=jnp.float32)
        source = (me + count_ep - 2 * step) % count_ep
        share = jnp.concatenate(
            [
                lax.dynamic_index_in_dim(weight, source, 0, keepdims=False),
                lax.dynamic_index_in_dim(weight, source ^ 1, 0, keepdims=False),
            ]
        )[:, None]
        terms = jnp.where(share > 0.0, share * expert_out, 0.0).astype(jnp.bfloat16)
        return terms[:rows], terms[rows:]

    running = None
    for step in list(range(1, ring)) + [0]:
        own, other = terms_of(step)
        total = own.astype(jnp.float32) + lax.ppermute(other, "ep", pair_swap).astype(jnp.float32)
        if running is not None:
            total = total + lax.ppermute(running, "ep", ring_step).astype(jnp.float32)
        running = total.astype(jnp.bfloat16)
    combined = total
    scale = lax.rsqrt(jnp.mean(combined * combined, axis=1, keepdims=True) + epsilon)
    mixed = (combined * scale * gain_full).astype(jnp.bfloat16)
    return lax.all_to_all(mixed, "tp", split_axis=1, concat_axis=0, tiled=True)


END, MID = 0, 1
INW, OUTW, PAIR = 0, 1, 2
LINE = 4
QUARTERS = 4
SLOTS = 14


def send_tables():
    sends = {(k, l): {} for k in (END, MID) for l in (INW, OUTW, PAIR)}
    for q in range(QUARTERS):
        sends[END, INW][q] = ("O", 0, q)
        sends[END, INW][4 + q] = ("P", 0, q)
        sends[END, PAIR][q] = ("O", 0, q)
        sends[END, PAIR][6 + q] = ("O", 2, q)
        sends[END, PAIR][10 + q] = ("O", 3, q)
        sends[MID, OUTW][q] = ("O", 1, q)
        sends[MID, OUTW][4 + q] = ("O", 2, q)
        sends[MID, OUTW][8 + q] = ("O", 3, q)
        sends[MID, INW][q] = ("O", 1, q)
        sends[MID, INW][4 + q] = ("O", 0, q)
        for b in (1, 2, 3):
            sends[MID, PAIR][4 * (b - 1) + q] = ("O", b, q)
    for q in (0, 1):
        sends[END, PAIR][4 + q] = ("O", 1, q)
        sends[MID, OUTW][12 + q] = ("P", 1, 2 + q)
    return sends


def seen_from_far(sends):
    other = {"O": "P", "P": "O"}
    cross = lambda p: (other[p[0]], p[1], p[2])
    mirror = lambda p: (p[0], LINE - 1 - p[1], p[2])
    return {
        (END, INW): dict(sends[MID, OUTW]),
        (END, OUTW): {},
        (END, PAIR): {s: cross(p) for s, p in sends[END, PAIR].items()},
        (MID, INW): {s: mirror(p) for s, p in sends[MID, INW].items()},
        (MID, OUTW): dict(sends[END, INW]),
        (MID, PAIR): {s: cross(p) for s, p in sends[MID, PAIR].items()},
    }


def pieces(first, *names):
    return {first + i: (n[0], int(n[1]), int(n[2])) for i, n in enumerate(names)}


SENDS = send_tables()
RECVS = seen_from_far(SENDS)
LONG = ("P23", "P33", "P32", "P31", "P30", "P22", "P21", "P20", "P11", "P10")
BACK_SENDS = {
    (END, PAIR): pieces(0, *LONG, "P03", "P02", "P01", "P00"),
    (END, INW): pieces(
        0, "O13", "O12", "O23", "O33", "O32", "O31", "O30", "O22", "O21", "O20", "P13", "P12", "O11", "O10"
    ),
    (END, OUTW): {},
    (MID, PAIR): {**pieces(0, *LONG), **pieces(12, "P13", "P12")},
    (MID, INW): pieces(4, "O23", "O33", "O32", "O31", "O30", "O22", "O21", "O20"),
    (MID, OUTW): {**pieces(3, "P03", "P02", "P01", "P00"), **pieces(7, "O03", "O02", "O01", "O00")},
}
BACK_RECVS = seen_from_far(BACK_SENDS)
ORDER = {
    END: [("O", 0), ("P", 0), ("O", 1), ("O", 2), ("P", 2), ("O", 3), ("P", 1), ("P", 3)],
    MID: [("O", 1), ("O", 0), ("O", 2), ("P", 1), ("P", 2), ("O", 3), ("P", 0), ("P", 3)],
}


def children(kind, piece):
    return [(l, s) for l in (INW, OUTW, PAIR) for s, p in BACK_RECVS[kind, l].items() if p == piece]


def fused_kernel(
    tok_ref, gain_ref, dense_ref, gate_ref, up_ref, down_ref, out_ref, scale_ref,
    tok_buf, xs, wg, wu, wd, hid, rin, rout, fin, squares, turned_scale, wts, wcol,
    local_sem, w_send, w_recv, m_send, m_recv, d_send, d_recv, r_send, r_recv, f_send, f_recv, s_send, s_recv,
):
    me, tp = lax.axis_index("ep"), lax.axis_index("tp")
    count_ep, rows, width = xs.shape
    count_tp = wg.shape[0]
    part = wg.shape[2]
    quarter = width // QUARTERS
    piece_rows = rows // QUARTERS
    none = rin.shape[0] - 1
    z, y = me // 2, me % 2
    low = z < LINE // 2
    is_end = (z == 0) | (z == LINE - 1)
    is_mid = jnp.logical_not(is_end)
    pick = lambda a, b: jnp.where(is_end, a, b)
    inward = jnp.where(low, z + 1, z - 1) * 2 + y
    outward = jnp.where(low, z - 1, z + 1) * 2 + y
    pair = z * 2 + 1 - y
    links = (inward, outward, pair)
    far_link = (pick(OUTW, INW), INW, PAIR)

    def block_of(column, b):
        line = jnp.where(low, b, LINE - 1 - b)
        return line * 2 + (y if column == "O" else 1 - y)

    def for_kinds(table, body):
        if END in table and MID in table:
            body(table[END], table[MID])
        elif END in table:
            pl.when(is_end)(lambda: body(table[END], table[END]))
        elif MID in table:
            pl.when(is_mid)(lambda: body(table[MID], table[MID]))

    def place(a, b):
        block = pick(block_of(a[0], a[1]), block_of(b[0], b[1]))
        return block, pick(a[2], b[2]) if a[2] != b[2] else a[2]

    def at(table, link, s):
        return {k: table[k, link][s] for k in (END, MID) if s in table[k, link]}

    def remote(src, dst, send, recv, ep, to):
        return pltpu.make_async_remote_copy(
            src_ref=src, dst_ref=dst, send_sem=send, recv_sem=recv, device_id=(ep, to), device_id_type=MESH
        )

    items = [(gate_ref, lambda owner: wg.at[owner]), (up_ref, lambda owner: wu.at[owner])]
    for q in reversed(range(QUARTERS)):
        items.append((down_ref.at[:, pl.ds(q * quarter, quarter)], lambda owner, q=q: wd.at[q, owner]))
    GATE, UP = 0, 1
    DOWN = {q: 2 + n for n, q in enumerate(reversed(range(QUARTERS)))}

    own_rows = pltpu.make_async_copy(tok_ref.at[pl.ds(tp * rows, rows)], tok_buf, local_sem.at[len(items)])
    own_rows.start()
    mine = [pltpu.make_async_copy(src, dst(tp), local_sem.at[i]) for i, (src, dst) in enumerate(items)]
    for copy in mine:
        copy.start()

    barrier = pltpu.get_barrier_semaphore()
    for step in range(1, count_ep):
        pl.semaphore_signal(barrier, inc=1, device_id=(lax.rem(me + step, count_ep), tp), device_id_type=MESH)
    for step in range(1, count_tp):
        pl.semaphore_signal(barrier, inc=1, device_id=(me, lax.rem(tp + step, count_tp)), device_id_type=MESH)

    own_rows.wait()
    group = 16

    def norm(i, carry):
        at_rows = pl.ds(pl.multiple_of(i * group, group), group)
        value = tok_buf[at_rows, :].astype(jnp.float32)
        scale = lax.rsqrt(jnp.mean(value * value, axis=1, keepdims=True) + epsilon)
        xs[me, at_rows, :] = (value * scale * gain_ref[...]).astype(jnp.bfloat16)
        return carry

    lax.fori_loop(0, rows // group, norm, 0)
    pl.semaphore_wait(barrier, count_ep + count_tp - 2)

    near, far = tp + 1 - 2 * (tp % 2), lax.rem(tp + 2, count_tp)
    diagonal = far + 1 - 2 * (far % 2)
    OVER, NEAR, ONWARD = 0, 1, 2

    def weight_copy(way, i, src, owner, target):
        return remote(src, items[i][1](owner), w_send.at[way, i], w_recv.at[way, i], me, target)

    over_x = [weight_copy(OVER, i, src, tp, far) for i, (src, _) in enumerate(items)]
    to_near = [weight_copy(NEAR, i, src, tp, near) for i, (src, _) in enumerate(items)]
    onward = [weight_copy(ONWARD, i, dst(far), far, near) for i, (_, dst) in enumerate(items)]
    in_x = [weight_copy(OVER, i, dst(far), far, far) for i, (_, dst) in enumerate(items)]
    in_near = [weight_copy(NEAR, i, dst(near), near, near) for i, (_, dst) in enumerate(items)]
    in_onward = [weight_copy(ONWARD, i, dst(diagonal), diagonal, near) for i, (_, dst) in enumerate(items)]

    def pass_on(i):
        in_x[i].wait_recv()
        onward[i].start()

    def mix_copy(step):
        return remote(
            dense_ref, wts.at[me], m_send.at[step - 1], m_recv.at[step - 1], lax.rem(me + step, count_ep), tp
        )

    def mix_wait(step):
        source = lax.rem(me + count_ep - step, count_ep)
        remote(dense_ref, wts.at[source], m_send.at[step - 1], m_recv.at[step - 1], source, tp).wait_recv()

    def row_copy(link, s, piece, arrival=False):
        block, q = piece
        ref = xs.at[block, pl.ds(q * piece_rows, piece_rows)]
        known = link if arrival else far_link[link]
        return remote(ref, ref, d_send.at[link, s], d_recv.at[known, s], links[link], tp)

    order = [pick(block_of(*ORDER[END][k]), block_of(*ORDER[MID][k])) for k in range(count_ep)]

    def ordered(k):
        block = order[0]
        for i in range(1, count_ep):
            block = jnp.where(k == i, order[i], block)
        return block

    def gate_up(first, last, sources):
        def body(i, carry):
            block = ordered(first + i // len(sources))
            source = sources[0]
            for n in range(1, len(sources)):
                source = jnp.where(i % len(sources) == n, sources[n], source)
            x = xs[block]
            gate = jnp.dot(x, wg[source], preferred_element_type=jnp.float32)
            up = jnp.dot(x, wu[source], preferred_element_type=jnp.float32)
            hidden = gate / (1.0 + jnp.exp(-gate)) * up
            hid[block, :, pl.ds(pl.multiple_of(source * part, part), part)] = hidden.astype(jnp.bfloat16)
            return carry

        lax.fori_loop(0, (last - first) * len(sources), body, 0)

    def dispatch_sends(s):
        for link in (INW, OUTW, PAIR):
            for_kinds(at(SENDS, link, s), lambda a, b: row_copy(link, s, place(a, b)).start())

    def dispatch_waits(s):
        for link in (INW, OUTW, PAIR):
            for_kinds(at(RECVS, link, s), lambda a, b: row_copy(link, s, place(a, b), True).wait_recv())

    chip, other_chip = (tp, near), (far, diagonal)

    for s in range(SLOTS):
        if s >= 2:
            dispatch_waits(s - 2)
        dispatch_sends(s)
        if s == 0:
            for copy in over_x:
                copy.start()
            for copy in to_near:
                copy.start()
        if s == 1:
            wts[me] = dense_ref[...]
            for step in range(1, count_ep):
                mix_copy(step).start()
            for i in (GATE, UP):
                mine[i].wait()
                in_near[i].wait_recv()
            gate_up(0, 1, chip)
        if s == 5:
            gate_up(1, 2, chip)
        if s == 6:
            gate_up(2, 3, chip)
        if s == 7:
            pass_on(GATE)
            for step in range(1, count_ep):
                mix_wait(step)
            for block in range(count_ep):
                turned = jnp.transpose(wts[block])
                lane = lax.broadcasted_iota(jnp.int32, turned.shape, 1)
                column = jnp.sum(jnp.where(lane == me, turned, 0.0), axis=1, keepdims=True)
                wcol[block] = jnp.broadcast_to(column[:rows], (rows, 128))
        if s == 8:
            rin[none] = jnp.zeros(rin.shape[1:], rin.dtype)
            squares[...] = jnp.zeros_like(squares)
        if s == 9:
            gate_up(3, 4, chip)
        if s == 11:
            gate_up(4, 5, chip)
        if s == 12:
            pass_on(UP)
            in_onward[GATE].wait_recv()
            in_onward[UP].wait_recv()
            gate_up(0, 3, other_chip)
        if s == 13:
            pass_on(DOWN[3])
            gate_up(5, 6, chip)
            gate_up(4, 5, other_chip)

    def down(block, q):
        value = jnp.dot(
            hid[block], wd[q].reshape(count_tp * part, quarter), preferred_element_type=jnp.float32
        )
        share = jnp.concatenate([wcol[block]] * (quarter // 128), axis=1)
        return jnp.where(share > 0.0, share * value, 0.0)

    def back_copy(link, s):
        return remote(
            rout.at[link * SLOTS + s], rin.at[far_link[link] * SLOTS + s],
            r_send.at[link, s], r_recv.at[far_link[link], s], links[link], tp,
        )

    def back_wait(link, s):
        here = rin.at[link * SLOTS + s]
        remote(here, here, r_send.at[link, s], r_recv.at[link, s], links[link], tp).wait_recv()

    def wait_children(kids):
        shared = [c for c in kids.get(END, []) if len(kids) == 1 or c in kids.get(MID, [])]
        if len(kids) == 1:
            shared = next(iter(kids.values()))
        for c in shared:
            back_wait(*c)
        for kind, cond in ((END, is_end), (MID, is_mid)):
            extra = [c for c in kids.get(kind, []) if c not in shared]
            if extra:
                def waits(extra=extra):
                    for c in extra:
                        back_wait(*c)
                pl.when(cond)(waits)

    def arrived(kids):
        indices = []
        for n in range(max(len(v) for v in kids.values())):
            ids = [v[n][0] * SLOTS + v[n][1] if n < len(v) else none for v in kids.values()]
            indices.append(ids[0] if len(set(ids)) == 1 else pick(*ids))
        return indices

    def total_of(table):
        kids = {k: children(k, p) for k, p in table.items()}
        wait_children(kids)
        values = list(table.values())
        total = down(*place(values[0], values[-1]))
        for index in arrived(kids):
            total = total + rin[index].astype(jnp.float32)
        return total

    def back_slot(link, s):
        table = at(BACK_SENDS, link, s)

        def body(*_):
            rout[link * SLOTS + s] = total_of(table).astype(jnp.bfloat16)
            back_copy(link, s).start()

        for_kinds(table, body)

    def ready(q):
        i = DOWN[q]
        mine[i].wait()
        in_near[i].wait_recv()
        in_onward[i].wait_recv()

    def final_copy(q, source):
        return remote(fin.at[q], out_ref.at[source], f_send.at[q], f_recv.at[source], me, q)

    def finish(q):
        total = total_of({END: ("O", 0, q), MID: ("O", 1, q)})
        square = total * total
        lanes = squares.shape[1]
        squares[...] += sum(square[:, i:i + lanes] for i in range(0, quarter, lanes))
        fin[q] = total.astype(jnp.bfloat16)
        pl.when(tp != q)(lambda: final_copy(q, tp).start())

    def keep(q):
        return pltpu.make_async_copy(fin.at[q], out_ref.at[q], local_sem.at[0])

    ready(3)
    dispatch_waits(SLOTS - 2)
    for r in range(SLOTS + 2):
        if r == 1:
            dispatch_waits(SLOTS - 1)
            pass_on(DOWN[2])
            gate_up(7, 8, chip + other_chip)
            ready(2)
        if r == 2:
            pass_on(DOWN[1])
            gate_up(3, 4, other_chip)
            gate_up(5, 6, other_chip)
        if r == 3:
            pass_on(DOWN[0])
            gate_up(6, 7, chip + other_chip)
            ready(1)
        if r == 4:
            ready(0)
        if r < SLOTS:
            for link in (PAIR, INW, OUTW):
                back_slot(link, r)
        if r >= SLOTS - 2:
            finish(SLOTS + 1 - r)

    mean = jnp.sum(squares[...], axis=1, keepdims=True) / width
    scale = jnp.broadcast_to(lax.rsqrt(mean + epsilon), squares.shape)
    turned_scale[:, :rows] = jnp.transpose(scale)[:turned_scale.shape[0], :]

    def scale_copy(step):
        return remote(
            turned_scale, scale_ref.at[tp], s_send.at[step - 1], s_recv.at[step - 1],
            me, lax.rem(tp + step, count_tp),
        )

    def scale_wait(step):
        source = lax.rem(tp + count_tp - step, count_tp)
        remote(
            turned_scale, scale_ref.at[source], s_send.at[step - 1], s_recv.at[step - 1], me, source
        ).wait_recv()

    for step in range(1, count_tp):
        scale_copy(step).start()
    keep_scale = pltpu.make_async_copy(turned_scale, scale_ref.at[tp], local_sem.at[1])
    keep_scale.start()
    keep(tp).start()

    for link in (INW, OUTW, PAIR):
        for s in range(SLOTS):
            for_kinds(at(SENDS, link, s), lambda a, b: row_copy(link, s, place(a, b)).wait_send())
            for_kinds(at(BACK_SENDS, link, s), lambda a, b: back_copy(link, s).wait_send())
    for copies in (over_x, to_near, onward):
        for copy in copies:
            copy.wait_send()
    for step in range(1, count_ep):
        mix_copy(step).wait_send()
    for step in range(1, count_tp):
        scale_copy(step).wait_send()
        scale_wait(step)
        source = lax.rem(tp + step, count_tp)
        remote(fin.at[tp], out_ref.at[source], f_send.at[tp], f_recv.at[source], me, source).wait_recv()
    for q in range(QUARTERS):
        pl.when(tp != q)(lambda: final_copy(q, tp).wait_send())
    keep(tp).wait()
    keep_scale.wait()


def fused(tokens, in_gain, route_ids, route_scores, gate_weight, up_weight, down_weight, out_gain):
    count_ep, count_tp = lax.axis_size("ep"), lax.axis_size("tp")
    experts = count_ep * gate_weight.shape[0]
    tok_count, width = tokens.shape
    rows = tok_count // count_tp
    part = gate_weight.shape[2]
    quarter = width // QUARTERS
    start = lax.axis_index("tp") * rows
    ids = lax.dynamic_slice_in_dim(route_ids, start, rows, 0)
    scores = lax.dynamic_slice_in_dim(route_scores, start, rows, 0)
    mix = scores / jnp.sum(scores, axis=1, keepdims=True)
    chosen = ids[:, :, None] == jnp.arange(experts, dtype=jnp.int32)[None, None, :]
    dense = jnp.sum(jnp.where(chosen, mix[:, :, None], 0.0), axis=1).T
    lanes = -(-rows // 128) * 128
    dense = jnp.pad(dense, ((0, 0), (0, lanes - rows)))
    bf16, f32 = jnp.bfloat16, jnp.float32
    dma = pltpu.SemaphoreType.DMA
    any_space = pl.BlockSpec(memory_space=pltpu.HBM)
    in_vmem = pl.BlockSpec(memory_space=pltpu.VMEM)
    weights = 2 + QUARTERS
    out, scale = pl.pallas_call(
        fused_kernel,
        name="experts",
        out_shape=(
            jax.ShapeDtypeStruct((count_tp, rows, quarter), bf16),
            jax.ShapeDtypeStruct((count_tp, 8, lanes), f32),
        ),
        in_specs=[any_space, in_vmem, in_vmem, any_space, any_space, any_space],
        out_specs=(any_space, any_space),
        scratch_shapes=[
            pltpu.VMEM((rows, width), bf16),
            pltpu.VMEM((count_ep, rows, width), bf16),
            pltpu.VMEM((count_tp, width, part), bf16),
            pltpu.VMEM((count_tp, width, part), bf16),
            pltpu.VMEM((QUARTERS, count_tp, part, quarter), bf16),
            pltpu.VMEM((count_ep, rows, part * count_tp), bf16),
            pltpu.VMEM((3 * SLOTS + 1, rows, quarter), bf16),
            pltpu.VMEM((3 * SLOTS, rows, quarter), bf16),
            pltpu.VMEM((QUARTERS, rows, quarter), bf16),
            pltpu.VMEM((rows, 128), f32),
            pltpu.VMEM((8, lanes), f32),
            pltpu.VMEM((count_ep, experts, lanes), f32),
            pltpu.VMEM((count_ep, rows, 128), f32),
            dma((weights + 1,)),
            dma((3, weights)),
            dma((3, weights)),
            dma((count_ep - 1,)),
            dma((count_ep - 1,)),
            dma((3, SLOTS)),
            dma((3, SLOTS)),
            dma((3, SLOTS)),
            dma((3, SLOTS)),
            dma((QUARTERS,)),
            dma((count_tp,)),
            dma((count_tp - 1,)),
            dma((count_tp - 1,)),
        ],
        compiler_params=pltpu.CompilerParams(
            collective_id=0, has_side_effects=True, vmem_limit_bytes=63 * 2**20
        ),
    )(tokens, in_gain.reshape(1, width), dense, gate_weight[0], up_weight[0], down_weight[0])
    out = out.astype(f32) * scale[:, 0, :rows][:, :, None] * out_gain
    return out.astype(bf16).reshape(tok_count, quarter)


def solution(mesh):
    in_specs = (
        P("ep", None),
        P(),
        P("ep", None),
        P("ep", None),
        P("ep", None, "tp"),
        P("ep", None, "tp"),
        P("ep", "tp", None),
        P("tp"),
    )
    out_specs = P("ep", "tp")
    small = mesh.shape["ep"] == 2 * LINE and mesh.shape["tp"] == QUARTERS
    return jax.shard_map(
        fused if small else per_device, mesh=mesh, in_specs=in_specs, out_specs=out_specs, check_vma=False
    )
```

```python
import functools

import jax
import jax.numpy as jnp
from jax import lax
from jax.experimental import pallas as pl
from jax.experimental.pallas import tpu as pltpu
from jax.sharding import PartitionSpec as P

epsilon = 1e-06
MESH = pl.DeviceIdType.MESH


def gathered(block, count):
    blocks = [block]
    bit = 1
    swaps = []
    while bit < count:
        swaps.append([(i, i ^ bit) for i in range(count)])
        bit *= 2
    first = lax.ppermute(block, "tp", swaps[0])
    blocks.append(first)
    for pairs in swaps[1:]:
        far = lax.ppermute(block, "tp", pairs)
        blocks.append(far)
        blocks.append(lax.ppermute(far, "tp", swaps[0]))
    return blocks


def per_device(
    tokens, in_gain, route_ids, route_scores, gate_weight, up_weight, down_weight, out_gain
):
    count_ep = lax.axis_size("ep")
    count_tp = lax.axis_size("tp")
    experts = count_ep * gate_weight.shape[0]
    tok_count, full_width = tokens.shape
    rows = tok_count // count_tp
    start = lax.axis_index("tp") * rows
    gates = gathered(gate_weight[0], count_tp)
    ups = gathered(up_weight[0], count_tp)
    downs = gathered(down_weight[0], count_tp)
    gain_full = lax.all_gather(out_gain, "tp", axis=0, tiled=True)

    as_float = lax.dynamic_slice_in_dim(tokens, start, rows, 0).astype(jnp.float32)
    normed = (
        as_float
        * lax.rsqrt(jnp.mean(as_float * as_float, axis=1, keepdims=True) + epsilon)
        * in_gain
    ).astype(jnp.bfloat16)
    ring = count_ep // 2
    pair_swap = [(i, i ^ 1) for i in range(count_ep)]
    ring_step = [(i, (i + 2) % count_ep) for i in range(count_ep)]
    held = [normed]
    for _ in range(1, ring):
        held.append(lax.ppermute(held[-1], "ep", ring_step))
    partner = [lax.ppermute(block, "ep", pair_swap) for block in held]

    ids = lax.dynamic_slice_in_dim(route_ids, start, rows, 0)
    scores = lax.dynamic_slice_in_dim(route_scores, start, rows, 0)
    mix = scores / jnp.sum(scores, axis=1, keepdims=True)
    chosen = ids[:, :, None] == jnp.arange(experts, dtype=jnp.int32)[None, None, :]
    dense = jnp.sum(jnp.where(chosen, mix[:, :, None], 0.0), axis=1).T
    weight = lax.all_to_all(dense, "ep", split_axis=0, concat_axis=0, tiled=True).reshape(count_ep, rows)

    gates, ups, held = lax.optimization_barrier((gates, ups, held))
    gate_full = jnp.concatenate(gates, 1)
    up_full = jnp.concatenate(ups, 1)
    down_full = jnp.concatenate(downs, 0)
    me = lax.axis_index("ep")

    def terms_of(step):
        block = jnp.concatenate([held[step], partner[step]], 0)
        gate_acts = jnp.dot(block, gate_full, preferred_element_type=jnp.float32)
        up_acts = jnp.dot(block, up_full, preferred_element_type=jnp.float32)
        hidden = (jax.nn.silu(gate_acts) * up_acts).astype(jnp.bfloat16)
        expert_out = jnp.dot(hidden, down_full, preferred_element_type=jnp.float32)
        source = (me + count_ep - 2 * step) % count_ep
        share = jnp.concatenate(
            [
                lax.dynamic_index_in_dim(weight, source, 0, keepdims=False),
                lax.dynamic_index_in_dim(weight, source ^ 1, 0, keepdims=False),
            ]
        )[:, None]
        terms = jnp.where(share > 0.0, share * expert_out, 0.0).astype(jnp.bfloat16)
        return terms[:rows], terms[rows:]

    running = None
    for step in list(range(1, ring)) + [0]:
        own, other = terms_of(step)
        total = own.astype(jnp.float32) + lax.ppermute(other, "ep", pair_swap).astype(jnp.float32)
        if running is not None:
            total = total + lax.ppermute(running, "ep", ring_step).astype(jnp.float32)
        running = total.astype(jnp.bfloat16)
    combined = total
    scale = lax.rsqrt(jnp.mean(combined * combined, axis=1, keepdims=True) + epsilon)
    mixed = (combined * scale * gain_full).astype(jnp.bfloat16)
    return lax.all_to_all(mixed, "tp", split_axis=1, concat_axis=0, tiled=True)


END, MID = 0, 1
INW, OUTW, PAIR = 0, 1, 2
LINE = 4
QUARTERS = 4
SLOTS = 15
BACK = 14
BACK_START = 13


def seen_from_far(sends):
    other = {"O": "P", "P": "O"}
    cross = lambda p: (other[p[0]], p[1], p[2])
    mirror = lambda p: (p[0], LINE - 1 - p[1], p[2])
    return {
        (END, INW): dict(sends[MID, OUTW]),
        (END, OUTW): {},
        (END, PAIR): {s: cross(p) for s, p in sends[END, PAIR].items()},
        (MID, INW): {s: mirror(p) for s, p in sends[MID, INW].items()},
        (MID, OUTW): dict(sends[END, INW]),
        (MID, PAIR): {s: cross(p) for s, p in sends[MID, PAIR].items()},
    }


def pieces(first, *names):
    return {first + i: (n[0], int(n[1]), int(n[2])) for i, n in enumerate(names)}


FOUR = range(QUARTERS)
SENDS = {
    (END, INW): pieces(0, *(f"O0{q}" for q in FOUR), *(f"P0{q}" for q in FOUR)),
    (END, OUTW): {},
    (END, PAIR): pieces(0, *(f"O{b}{q}" for b in (0, 2, 3) for q in FOUR), "O10"),
    (MID, INW): pieces(0, *(f"O{b}{q}" for b in (1, 0) for q in FOUR)),
    (MID, OUTW): pieces(
        0, "O10", "O11", *(f"O{b}{q}" for b in (2, 3) for q in FOUR), "O12", "O13", "P11", "P12", "P13"
    ),
    (MID, PAIR): pieces(0, *(f"O{b}{q}" for b in (1, 2, 3) for q in FOUR)),
}
RECVS = seen_from_far(SENDS)
LONG = ("P23", "P33", "P32", "P31", "P30", "P22", "P21", "P20", "P11", "P10")
BACK_SENDS = {
    (END, PAIR): pieces(0, *LONG, "P03", "P02", "P01", "P00"),
    (END, INW): pieces(
        0, "O13", "O12", "O23", "O33", "O32", "O31", "O30", "O22", "O21", "O20", "P13", "P12", "O11", "O10"
    ),
    (END, OUTW): {},
    (MID, PAIR): {**pieces(0, *LONG), **pieces(12, "P13", "P12")},
    (MID, INW): pieces(4, "O23", "O33", "O32", "O31", "O30", "O22", "O21", "O20"),
    (MID, OUTW): pieces(4, "P03", "P02", "P01", "O03", "O02", "O01", "O00", "P00"),
}
BACK_RECVS = seen_from_far(BACK_SENDS)
ORDER = {
    END: [("O", 0), ("P", 0), ("O", 2), ("P", 2), ("O", 3), ("O", 1), ("P", 3), ("P", 1)],
    MID: [("O", 1), ("O", 0), ("O", 2), ("P", 2), ("O", 3), ("P", 1), ("P", 3), ("P", 0)],
}


def children(kind, piece):
    return [(l, s) for l in (INW, OUTW, PAIR) for s, p in BACK_RECVS[kind, l].items() if p == piece]


def fused_kernel(
    tok_ref, gain_ref, ids_ref, scores_ref, gate_ref, up_ref, down_ref, out_ref, scale_ref,
    tok_buf, xs, wg, wu, wd, hid, rin, rout, fin, squares, turned_scale, dense_ref, wts, wcol,
    local_sem, w_send, w_recv, m_send, m_recv, d_send, d_recv, r_send, r_recv, f_send, f_recv, s_send, s_recv,
):
    me, tp = lax.axis_index("ep"), lax.axis_index("tp")
    count_ep, rows, width = xs.shape
    count_tp = wg.shape[0]
    part = wg.shape[2]
    quarter = width // QUARTERS
    piece_rows = rows // QUARTERS
    none = rin.shape[0] - 1
    z, y = me // 2, me % 2
    low = z < LINE // 2
    is_end = (z == 0) | (z == LINE - 1)
    is_mid = jnp.logical_not(is_end)
    pick = lambda a, b: jnp.where(is_end, a, b)
    inward = jnp.where(low, z + 1, z - 1) * 2 + y
    outward = jnp.where(low, z - 1, z + 1) * 2 + y
    pair = z * 2 + 1 - y
    links = (inward, outward, pair)
    far_link = (pick(OUTW, INW), INW, PAIR)

    def block_of(column, b):
        line = jnp.where(low, b, LINE - 1 - b)
        return line * 2 + (y if column == "O" else 1 - y)

    def for_kinds(table, body):
        if END in table and MID in table:
            body(table[END], table[MID])
        elif END in table:
            pl.when(is_end)(lambda: body(table[END], table[END]))
        elif MID in table:
            pl.when(is_mid)(lambda: body(table[MID], table[MID]))

    def place(a, b):
        block = pick(block_of(a[0], a[1]), block_of(b[0], b[1]))
        return block, pick(a[2], b[2]) if a[2] != b[2] else a[2]

    def at(table, link, s):
        return {k: table[k, link][s] for k in (END, MID) if s in table[k, link]}

    def remote(src, dst, send, recv, ep, to):
        return pltpu.make_async_remote_copy(
            src_ref=src, dst_ref=dst, send_sem=send, recv_sem=recv, device_id=(ep, to), device_id_type=MESH
        )

    items = [(gate_ref, lambda owner: wg.at[owner]), (up_ref, lambda owner: wu.at[owner])]
    for q in reversed(range(QUARTERS)):
        items.append((down_ref.at[:, pl.ds(q * quarter, quarter)], lambda owner, q=q: wd.at[q, owner]))
    GATE, UP = 0, 1
    DOWN = {q: 2 + n for n, q in enumerate(reversed(range(QUARTERS)))}

    own_rows = pltpu.make_async_copy(tok_ref.at[pl.ds(tp * rows, rows)], tok_buf, local_sem.at[len(items)])
    own_rows.start()
    mine = [pltpu.make_async_copy(src, dst(tp), local_sem.at[i]) for i, (src, dst) in enumerate(items)]
    for copy in mine:
        copy.start()

    barrier = pltpu.get_barrier_semaphore()
    for step in range(1, count_ep):
        pl.semaphore_signal(barrier, inc=1, device_id=(lax.rem(me + step, count_ep), tp), device_id_type=MESH)
    for step in range(1, count_tp):
        pl.semaphore_signal(barrier, inc=1, device_id=(me, lax.rem(tp + step, count_tp)), device_id_type=MESH)

    own_rows.wait()
    group = 16

    def norm(i, carry):
        at_rows = pl.ds(pl.multiple_of(i * group, group), group)
        value = tok_buf[at_rows, :].astype(jnp.float32)
        scale = lax.rsqrt(jnp.mean(value * value, axis=1, keepdims=True) + epsilon)
        xs[me, at_rows, :] = (value * scale * gain_ref[...]).astype(jnp.bfloat16)
        return carry

    lax.fori_loop(0, piece_rows // group, norm, 0)
    pl.semaphore_wait(barrier, count_ep + count_tp - 2)

    near, far = tp + 1 - 2 * (tp % 2), lax.rem(tp + 2, count_tp)
    diagonal = far + 1 - 2 * (far % 2)
    OVER, NEAR, ONWARD = 0, 1, 2

    def weight_copy(way, i, src, owner, target):
        return remote(src, items[i][1](owner), w_send.at[way, i], w_recv.at[way, i], me, target)

    over_x = [weight_copy(OVER, i, src, tp, far) for i, (src, _) in enumerate(items)]
    to_near = [weight_copy(NEAR, i, src, tp, near) for i, (src, _) in enumerate(items)]
    onward = [weight_copy(ONWARD, i, dst(far), far, near) for i, (_, dst) in enumerate(items)]
    in_x = [weight_copy(OVER, i, dst(far), far, far) for i, (_, dst) in enumerate(items)]
    in_near = [weight_copy(NEAR, i, dst(near), near, near) for i, (_, dst) in enumerate(items)]
    in_onward = [weight_copy(ONWARD, i, dst(diagonal), diagonal, near) for i, (_, dst) in enumerate(items)]

    def pass_on(i):
        in_x[i].wait_recv()
        onward[i].start()

    def mix_copy(step):
        return remote(
            dense_ref, wts.at[me], m_send.at[step - 1], m_recv.at[step - 1], lax.rem(me + step, count_ep), tp
        )

    def mix_wait(step):
        source = lax.rem(me + count_ep - step, count_ep)
        remote(dense_ref, wts.at[source], m_send.at[step - 1], m_recv.at[step - 1], source, tp).wait_recv()

    def row_copy(link, s, piece, arrival=False):
        block, q = piece
        ref = xs.at[block, pl.ds(q * piece_rows, piece_rows)]
        known = link if arrival else far_link[link]
        return remote(ref, ref, d_send.at[link, s], d_recv.at[known, s], links[link], tp)

    order = [pick(block_of(*ORDER[END][k]), block_of(*ORDER[MID][k])) for k in range(count_ep)]

    def ordered(k):
        block = order[0]
        for i in range(1, count_ep):
            block = jnp.where(k == i, order[i], block)
        return block

    def gate_up(first, last, sources):
        def body(i, carry):
            block = ordered(first + i // (len(sources) // 2))
            for n in (0, 1):
                source = sources[n]
                if len(sources) > 2:
                    source = jnp.where(i % 2 == 1, sources[2 + n], source)
                x = xs[block]
                gate = jnp.dot(x, wg[source], preferred_element_type=jnp.float32)
                up = jnp.dot(x, wu[source], preferred_element_type=jnp.float32)
                hidden = gate / (1.0 + jnp.exp(-gate)) * up
                hid[block, :, pl.ds(pl.multiple_of(source * part, part), part)] = hidden.astype(jnp.bfloat16)
            return carry

        lax.fori_loop(0, (last - first) * (len(sources) // 2), body, 0)

    def dispatch_sends(s):
        for link in (INW, OUTW, PAIR):
            for_kinds(at(SENDS, link, s), lambda a, b: row_copy(link, s, place(a, b)).start())

    def dispatch_waits(s):
        for link in (INW, OUTW, PAIR):
            for_kinds(at(RECVS, link, s), lambda a, b: row_copy(link, s, place(a, b), True).wait_recv())

    def down(block, q):
        value = jnp.dot(
            hid[block], wd[q].reshape(count_tp * part, quarter), preferred_element_type=jnp.float32
        )
        share = jnp.concatenate([wcol[block]] * (quarter // 128), axis=1)
        return jnp.where(share > 0.0, share * value, 0.0)

    def back_copy(link, s):
        return remote(
            rout.at[link * BACK + s], rin.at[far_link[link] * BACK + s],
            r_send.at[link, s], r_recv.at[far_link[link], s], links[link], tp,
        )

    def back_wait(link, s):
        here = rin.at[link * BACK + s]
        remote(here, here, r_send.at[link, s], r_recv.at[link, s], links[link], tp).wait_recv()

    def wait_children(kids):
        shared = [c for c in kids.get(END, []) if len(kids) == 1 or c in kids.get(MID, [])]
        if len(kids) == 1:
            shared = next(iter(kids.values()))
        for c in shared:
            back_wait(*c)
        for kind, cond in ((END, is_end), (MID, is_mid)):
            extra = [c for c in kids.get(kind, []) if c not in shared]
            if extra:
                def waits(extra=extra):
                    for c in extra:
                        back_wait(*c)

                pl.when(cond)(waits)

    def arrived(kids):
        indices = []
        for n in range(max(len(v) for v in kids.values())):
            ids = [v[n][0] * BACK + v[n][1] if n < len(v) else none for v in kids.values()]
            indices.append(ids[0] if len(set(ids)) == 1 else pick(*ids))
        return indices

    def total_of(table):
        kids = {k: children(k, p) for k, p in table.items()}
        wait_children(kids)
        values = list(table.values())
        total = down(*place(values[0], values[-1]))
        for index in arrived(kids):
            total = total + rin[index].astype(jnp.float32)
        return total

    def back_slot(link, s):
        table = at(BACK_SENDS, link, s)

        def body(*_):
            rout[link * BACK + s] = total_of(table).astype(jnp.bfloat16)
            back_copy(link, s).start()

        for_kinds(table, body)

    def ready(q):
        i = DOWN[q]
        mine[i].wait()
        in_near[i].wait_recv()
        in_onward[i].wait_recv()

    def final_copy(q, source):
        return remote(fin.at[q], out_ref.at[source], f_send.at[q], f_recv.at[source], me, q)

    def finish(q):
        total = total_of({END: ("O", 0, q), MID: ("O", 1, q)})
        square = total * total
        lanes = squares.shape[1]
        squares[...] += sum(square[:, i:i + lanes] for i in range(0, quarter, lanes))
        fin[q] = total.astype(jnp.bfloat16)
        pl.when(tp != q)(lambda: final_copy(q, tp).start())

    def keep(q):
        return pltpu.make_async_copy(fin.at[q], out_ref.at[q], local_sem.at[0])

    chip, other_chip = (tp, near), (far, diagonal)
    everyone = chip + other_chip
    links_back = (PAIR, INW, OUTW)

    for g in range(BACK_START + BACK + 2):
        if 2 <= g < SLOTS + 2:
            dispatch_waits(g - 2)
        if g == 0:
            over_x[GATE].start()
        if g < SLOTS:
            dispatch_sends(g)
        if g == 0:
            for copy in over_x[1:] + to_near:
                copy.start()
            lax.fori_loop(piece_rows // group, rows // group, norm, 0)
        if g == 1:
            expert = lax.broadcasted_iota(jnp.int32, (wts.shape[1], ids_ref.shape[1]), 0)
            tally = jnp.sum(scores_ref[...], axis=0, keepdims=True)
            dense = jnp.zeros(expert.shape, jnp.float32)
            for k in range(ids_ref.shape[0]):
                mix = scores_ref[k:k + 1, :] / tally
                dense = dense + jnp.where(ids_ref[k:k + 1, :] == expert, mix, 0.0)
            lanes = wts.shape[2]
            dense = jnp.concatenate([dense, jnp.zeros((dense.shape[0], lanes), jnp.float32)], axis=1)
            mine_only = dense[:, :lanes]
            for k in range(1, count_tp):
                mine_only = jnp.where(tp == k, dense[:, k * rows:k * rows + lanes], mine_only)
            dense_ref[...] = mine_only
            wts[me] = mine_only
            for step in range(1, count_ep):
                mix_copy(step).start()
            for i in (GATE, UP):
                mine[i].wait()
                in_near[i].wait_recv()
            gate_up(0, 1, chip)
        if g == 5:
            gate_up(1, 2, chip)
        if g == 6:
            rin[none] = jnp.zeros(rin.shape[1:], rin.dtype)
            squares[...] = jnp.zeros_like(squares)
        if g == 7:
            gate_up(2, 3, chip)
            pass_on(GATE)
        if g == 8:
            for step in range(1, count_ep):
                mix_wait(step)
            for block in range(count_ep):
                turned = jnp.transpose(wts[block])
                lane = lax.broadcasted_iota(jnp.int32, turned.shape, 1)
                column = jnp.sum(jnp.where(lane == me, turned, 0.0), axis=1, keepdims=True)
                wcol[block] = jnp.broadcast_to(column[:rows], (rows, 128))
        if g == 9:
            gate_up(3, 4, chip)
        if g == 11:
            gate_up(4, 5, chip)
        if g == 12:
            pass_on(UP)
            in_onward[GATE].wait_recv()
            in_onward[UP].wait_recv()
            gate_up(3, 4, other_chip)
            gate_up(2, 3, other_chip)
        if g < BACK_START:
            continue
        r = g - BACK_START
        if r == 0:
            pass_on(DOWN[3])
            ready(3)
            back_slot(PAIR, 0)
            gate_up(5, 6, everyone)
            back_slot(INW, 0)
            back_slot(OUTW, 0)
            continue
        if r == 1:
            gate_up(6, 7, everyone)
            back_slot(PAIR, 1)
            pass_on(DOWN[2])
            ready(2)
            back_slot(INW, 1)
            back_slot(OUTW, 1)
            gate_up(4, 5, other_chip)
            continue
        if r == 3:
            ready(1)
        if r == 4:
            ready(0)
        if r < BACK:
            for link in links_back:
                back_slot(link, r)
        if r == 2:
            gate_up(0, 2, other_chip)
            pass_on(DOWN[1])
        if r == 3:
            gate_up(7, 8, everyone)
            pass_on(DOWN[0])
        if r >= BACK - 2:
            finish(BACK + 1 - r)

    mean = jnp.sum(squares[...], axis=1, keepdims=True) / width
    scale = jnp.broadcast_to(lax.rsqrt(mean + epsilon), squares.shape)
    turned_scale[:, :rows] = jnp.transpose(scale)[:turned_scale.shape[0], :]

    def scale_copy(step):
        return remote(
            turned_scale, scale_ref.at[tp], s_send.at[step - 1], s_recv.at[step - 1],
            me, lax.rem(tp + step, count_tp),
        )

    def scale_wait(step):
        source = lax.rem(tp + count_tp - step, count_tp)
        remote(
            turned_scale, scale_ref.at[source], s_send.at[step - 1], s_recv.at[step - 1], me, source
        ).wait_recv()

    for step in range(1, count_tp):
        scale_copy(step).start()
    keep_scale = pltpu.make_async_copy(turned_scale, scale_ref.at[tp], local_sem.at[1])
    keep_scale.start()
    keep(tp).start()

    for link in (INW, OUTW, PAIR):
        for s in range(SLOTS):
            for_kinds(at(SENDS, link, s), lambda a, b: row_copy(link, s, place(a, b)).wait_send())
        for s in range(BACK):
            for_kinds(at(BACK_SENDS, link, s), lambda a, b: back_copy(link, s).wait_send())
    for copies in (over_x, to_near, onward):
        for copy in copies:
            copy.wait_send()
    for step in range(1, count_ep):
        mix_copy(step).wait_send()
    for step in range(1, count_tp):
        scale_copy(step).wait_send()
        scale_wait(step)
        source = lax.rem(tp + step, count_tp)
        remote(fin.at[tp], out_ref.at[source], f_send.at[tp], f_recv.at[source], me, source).wait_recv()
    for q in range(QUARTERS):
        pl.when(tp != q)(lambda: final_copy(q, tp).wait_send())
    keep(tp).wait()
    keep_scale.wait()


def fused(tokens, in_gain, route_ids, route_scores, gate_weight, up_weight, down_weight, out_gain):
    count_ep, count_tp = lax.axis_size("ep"), lax.axis_size("tp")
    experts = count_ep * gate_weight.shape[0]
    tok_count, width = tokens.shape
    rows = tok_count // count_tp
    part = gate_weight.shape[2]
    quarter = width // QUARTERS
    lanes = -(-rows // 128) * 128
    bf16, f32 = jnp.bfloat16, jnp.float32
    dma = pltpu.SemaphoreType.DMA
    any_space = pl.BlockSpec(memory_space=pltpu.HBM)
    in_vmem = pl.BlockSpec(memory_space=pltpu.VMEM)
    weights = 2 + QUARTERS
    out, scale = pl.pallas_call(
        fused_kernel,
        name="experts",
        out_shape=(
            jax.ShapeDtypeStruct((count_tp, rows, quarter), bf16),
            jax.ShapeDtypeStruct((count_tp, 8, lanes), f32),
        ),
        in_specs=[any_space, in_vmem, in_vmem, in_vmem, any_space, any_space, any_space],
        out_specs=(any_space, any_space),
        scratch_shapes=[
            pltpu.VMEM((rows, width), bf16),
            pltpu.VMEM((count_ep, rows, width), bf16),
            pltpu.VMEM((count_tp, width, part), bf16),
            pltpu.VMEM((count_tp, width, part), bf16),
            pltpu.VMEM((QUARTERS, count_tp, part, quarter), bf16),
            pltpu.VMEM((count_ep, rows, part * count_tp), bf16),
            pltpu.VMEM((3 * BACK + 1, rows, quarter), bf16),
            pltpu.VMEM((3 * BACK, rows, quarter), bf16),
            pltpu.VMEM((QUARTERS, rows, quarter), bf16),
            pltpu.VMEM((rows, 128), f32),
            pltpu.VMEM((8, lanes), f32),
            pltpu.VMEM((experts, lanes), f32),
            pltpu.VMEM((count_ep, experts, lanes), f32),
            pltpu.VMEM((count_ep, rows, 128), f32),
            dma((weights + 1,)),
            dma((3, weights)),
            dma((3, weights)),
            dma((count_ep - 1,)),
            dma((count_ep - 1,)),
            dma((3, SLOTS)),
            dma((3, SLOTS)),
            dma((3, BACK)),
            dma((3, BACK)),
            dma((QUARTERS,)),
            dma((count_tp,)),
            dma((count_tp - 1,)),
            dma((count_tp - 1,)),
        ],
        compiler_params=pltpu.CompilerParams(
            collective_id=0, has_side_effects=True, vmem_limit_bytes=63 * 2**20
        ),
    )(tokens, in_gain.reshape(1, width), route_ids.T, route_scores.T, gate_weight[0], up_weight[0], down_weight[0])
    out = out.astype(f32) * scale[:, 0, :rows][:, :, None] * out_gain
    return out.astype(bf16).reshape(tok_count, quarter)


def solution(mesh):
    in_specs = (
        P("ep", None),
        P(),
        P("ep", None),
        P("ep", None),
        P("ep", None, "tp"),
        P("ep", None, "tp"),
        P("ep", "tp", None),
        P("tp"),
    )
    out_specs = P("ep", "tp")
    small = mesh.shape["ep"] == 2 * LINE and mesh.shape["tp"] == QUARTERS
    return jax.shard_map(
        fused if small else per_device, mesh=mesh, in_specs=in_specs, out_specs=out_specs, check_vma=False
    )
```

```python
import functools

import jax
import jax.numpy as jnp
from jax import lax
from jax.experimental import pallas as pl
from jax.experimental.pallas import tpu as pltpu
from jax.sharding import PartitionSpec as P

epsilon = 1e-06
MESH = pl.DeviceIdType.MESH


def gathered(block, count):
    blocks = [block]
    bit = 1
    swaps = []
    while bit < count:
        swaps.append([(i, i ^ bit) for i in range(count)])
        bit *= 2
    first = lax.ppermute(block, "tp", swaps[0])
    blocks.append(first)
    for pairs in swaps[1:]:
        far = lax.ppermute(block, "tp", pairs)
        blocks.append(far)
        blocks.append(lax.ppermute(far, "tp", swaps[0]))
    return blocks


def per_device(
    tokens, in_gain, route_ids, route_scores, gate_weight, up_weight, down_weight, out_gain
):
    count_ep = lax.axis_size("ep")
    count_tp = lax.axis_size("tp")
    experts = count_ep * gate_weight.shape[0]
    tok_count, full_width = tokens.shape
    rows = tok_count // count_tp
    start = lax.axis_index("tp") * rows
    gates = gathered(gate_weight[0], count_tp)
    ups = gathered(up_weight[0], count_tp)
    downs = gathered(down_weight[0], count_tp)
    gain_full = lax.all_gather(out_gain, "tp", axis=0, tiled=True)

    as_float = lax.dynamic_slice_in_dim(tokens, start, rows, 0).astype(jnp.float32)
    normed = (
        as_float
        * lax.rsqrt(jnp.mean(as_float * as_float, axis=1, keepdims=True) + epsilon)
        * in_gain
    ).astype(jnp.bfloat16)
    ring = count_ep // 2
    pair_swap = [(i, i ^ 1) for i in range(count_ep)]
    ring_step = [(i, (i + 2) % count_ep) for i in range(count_ep)]
    held = [normed]
    for _ in range(1, ring):
        held.append(lax.ppermute(held[-1], "ep", ring_step))
    partner = [lax.ppermute(block, "ep", pair_swap) for block in held]

    ids = lax.dynamic_slice_in_dim(route_ids, start, rows, 0)
    scores = lax.dynamic_slice_in_dim(route_scores, start, rows, 0)
    mix = scores / jnp.sum(scores, axis=1, keepdims=True)
    chosen = ids[:, :, None] == jnp.arange(experts, dtype=jnp.int32)[None, None, :]
    dense = jnp.sum(jnp.where(chosen, mix[:, :, None], 0.0), axis=1).T
    weight = lax.all_to_all(dense, "ep", split_axis=0, concat_axis=0, tiled=True).reshape(count_ep, rows)

    gates, ups, held = lax.optimization_barrier((gates, ups, held))
    gate_full = jnp.concatenate(gates, 1)
    up_full = jnp.concatenate(ups, 1)
    down_full = jnp.concatenate(downs, 0)
    me = lax.axis_index("ep")

    def terms_of(step):
        block = jnp.concatenate([held[step], partner[step]], 0)
        gate_acts = jnp.dot(block, gate_full, preferred_element_type=jnp.float32)
        up_acts = jnp.dot(block, up_full, preferred_element_type=jnp.float32)
        hidden = (jax.nn.silu(gate_acts) * up_acts).astype(jnp.bfloat16)
        expert_out = jnp.dot(hidden, down_full, preferred_element_type=jnp.float32)
        source = (me + count_ep - 2 * step) % count_ep
        share = jnp.concatenate(
            [
                lax.dynamic_index_in_dim(weight, source, 0, keepdims=False),
                lax.dynamic_index_in_dim(weight, source ^ 1, 0, keepdims=False),
            ]
        )[:, None]
        terms = jnp.where(share > 0.0, share * expert_out, 0.0).astype(jnp.bfloat16)
        return terms[:rows], terms[rows:]

    running = None
    for step in list(range(1, ring)) + [0]:
        own, other = terms_of(step)
        total = own.astype(jnp.float32) + lax.ppermute(other, "ep", pair_swap).astype(jnp.float32)
        if running is not None:
            total = total + lax.ppermute(running, "ep", ring_step).astype(jnp.float32)
        running = total.astype(jnp.bfloat16)
    combined = total
    scale = lax.rsqrt(jnp.mean(combined * combined, axis=1, keepdims=True) + epsilon)
    mixed = (combined * scale * gain_full).astype(jnp.bfloat16)
    return lax.all_to_all(mixed, "tp", split_axis=1, concat_axis=0, tiled=True)


END, MID = 0, 1
INW, OUTW, PAIR = 0, 1, 2
LINE = 4
QUARTERS = 4
SLOTS = 15
BACK = 14
BACK_START = 13


def seen_from_far(sends):
    other = {"O": "P", "P": "O"}
    cross = lambda p: (other[p[0]], p[1], p[2])
    mirror = lambda p: (p[0], LINE - 1 - p[1], p[2])
    return {
        (END, INW): dict(sends[MID, OUTW]),
        (END, OUTW): {},
        (END, PAIR): {s: cross(p) for s, p in sends[END, PAIR].items()},
        (MID, INW): {s: mirror(p) for s, p in sends[MID, INW].items()},
        (MID, OUTW): dict(sends[END, INW]),
        (MID, PAIR): {s: cross(p) for s, p in sends[MID, PAIR].items()},
    }


def pieces(first, *names):
    return {first + i: (n[0], int(n[1]), int(n[2])) for i, n in enumerate(names)}


FOUR = range(QUARTERS)
SENDS = {
    (END, INW): pieces(0, *(f"O0{q}" for q in FOUR), *(f"P0{q}" for q in FOUR)),
    (END, OUTW): {},
    (END, PAIR): pieces(0, *(f"O{b}{q}" for b in (0, 2, 3) for q in FOUR), "O10"),
    (MID, INW): pieces(0, *(f"O{b}{q}" for b in (1, 0) for q in FOUR)),
    (MID, OUTW): pieces(
        0, "O10", "O11", *(f"O{b}{q}" for b in (2, 3) for q in FOUR), "O12", "O13", "P11", "P12", "P13"
    ),
    (MID, PAIR): pieces(0, *(f"O{b}{q}" for b in (1, 2, 3) for q in FOUR)),
}
RECVS = seen_from_far(SENDS)
LONG = ("P23", "P33", "P32", "P22", "P31", "P30", "P21", "P20", "P11", "P10")
BACK_SENDS = {
    (END, PAIR): pieces(0, *LONG, "P03", "P02", "P01", "P00"),
    (END, INW): pieces(
        0, "O13", "O12", "O23", "O33", "O32", "O22", "O31", "O30", "O21", "O20", "P13", "P12", "O11", "O10"
    ),
    (END, OUTW): {},
    (MID, PAIR): {**pieces(0, *LONG), **pieces(12, "P13", "P12")},
    (MID, INW): pieces(4, "O23", "O33", "O32", "O22", "O31", "O30", "O21", "O20"),
    (MID, OUTW): pieces(4, "P03", "P02", "P01", "O03", "O02", "P00", "O01", "O00"),
}
BACK_RECVS = seen_from_far(BACK_SENDS)
ORDER = {
    END: [("O", 0), ("P", 0), ("O", 2), ("P", 2), ("O", 3), ("O", 1), ("P", 3), ("P", 1)],
    MID: [("O", 1), ("O", 0), ("O", 2), ("P", 2), ("O", 3), ("P", 1), ("P", 3), ("P", 0)],
}


def children(kind, piece):
    return [(l, s) for l in (INW, OUTW, PAIR) for s, p in BACK_RECVS[kind, l].items() if p == piece]


def fused_kernel(
    tok_ref, gain_ref, ids_ref, scores_ref, out_gain_ref, gate_ref, up_ref, down_ref, out_ref,
    tok_buf, xs, wg, wu, wd, hid, rin, rout, fin, landed, stage, squares, scales, dense_ref, wts, wcol,
    local_sem, w_send, w_recv, m_send, m_recv, d_send, d_recv, r_send, r_recv, f_send, f_recv, s_send, s_recv,
):
    me, tp = lax.axis_index("ep"), lax.axis_index("tp")
    count_ep, rows, width = xs.shape
    count_tp = wg.shape[0]
    part = wg.shape[2]
    quarter = width // QUARTERS
    sub = width // count_tp // QUARTERS
    piece_rows = rows // QUARTERS
    none = rin.shape[0] - 1
    z, y = me // 2, me % 2
    low = z < LINE // 2
    is_end = (z == 0) | (z == LINE - 1)
    is_mid = jnp.logical_not(is_end)
    pick = lambda a, b: jnp.where(is_end, a, b)
    inward = jnp.where(low, z + 1, z - 1) * 2 + y
    outward = jnp.where(low, z - 1, z + 1) * 2 + y
    pair = z * 2 + 1 - y
    links = (inward, outward, pair)
    far_link = (pick(OUTW, INW), INW, PAIR)

    def block_of(column, b):
        line = jnp.where(low, b, LINE - 1 - b)
        return line * 2 + (y if column == "O" else 1 - y)

    def for_kinds(table, body):
        if END in table and MID in table:
            body(table[END], table[MID])
        elif END in table:
            pl.when(is_end)(lambda: body(table[END], table[END]))
        elif MID in table:
            pl.when(is_mid)(lambda: body(table[MID], table[MID]))

    def place(a, b):
        block = pick(block_of(a[0], a[1]), block_of(b[0], b[1]))
        return block, pick(a[2], b[2]) if a[2] != b[2] else a[2]

    def at(table, link, s):
        return {k: table[k, link][s] for k in (END, MID) if s in table[k, link]}

    def remote(src, dst, send, recv, ep, to):
        return pltpu.make_async_remote_copy(
            src_ref=src, dst_ref=dst, send_sem=send, recv_sem=recv, device_id=(ep, to), device_id_type=MESH
        )

    items = [(gate_ref, lambda owner: wg.at[owner]), (up_ref, lambda owner: wu.at[owner])]
    for q in reversed(range(QUARTERS)):
        items.append((wd.at[q, tp], lambda owner, q=q: wd.at[q, owner]))
    GATE, UP = 0, 1
    DOWN = {q: 2 + n for n, q in enumerate(reversed(range(QUARTERS)))}

    own_rows = pltpu.make_async_copy(tok_ref.at[pl.ds(tp * rows, rows)], tok_buf, local_sem.at[0])
    own_rows.start()
    mine = [
        pltpu.make_async_copy(gate_ref, wg.at[tp], local_sem.at[1]),
        pltpu.make_async_copy(up_ref, wu.at[tp], local_sem.at[2]),
    ]
    mine_down = [
        pltpu.make_async_copy(
            down_ref.at[:, pl.ds((c * QUARTERS + q) * sub, sub)],
            wd.at[q, tp, :, pl.ds(c * sub, sub)],
            local_sem.at[3 + q * count_tp + c],
        )
        for q in range(QUARTERS)
        for c in range(count_tp)
    ]
    for copy in mine + mine_down:
        copy.start()

    barrier = pltpu.get_barrier_semaphore()
    for step in range(1, count_ep):
        pl.semaphore_signal(barrier, inc=1, device_id=(lax.rem(me + step, count_ep), tp), device_id_type=MESH)
    for step in range(1, count_tp):
        pl.semaphore_signal(barrier, inc=1, device_id=(me, lax.rem(tp + step, count_tp)), device_id_type=MESH)

    own_rows.wait()
    group = 16

    def norm(i, carry):
        at_rows = pl.ds(pl.multiple_of(i * group, group), group)
        value = tok_buf[at_rows, :].astype(jnp.float32)
        scale = lax.rsqrt(jnp.mean(value * value, axis=1, keepdims=True) + epsilon)
        xs[me, at_rows, :] = (value * scale * gain_ref[...]).astype(jnp.bfloat16)
        return carry

    lax.fori_loop(0, piece_rows // group, norm, 0)
    pl.semaphore_wait(barrier, count_ep + count_tp - 2)

    near, far = tp + 1 - 2 * (tp % 2), lax.rem(tp + 2, count_tp)
    diagonal = far + 1 - 2 * (far % 2)
    OVER, NEAR, ONWARD = 0, 1, 2

    def weight_copy(way, i, src, owner, target):
        return remote(src, items[i][1](owner), w_send.at[way, i], w_recv.at[way, i], me, target)

    over_x = [weight_copy(OVER, i, src, tp, far) for i, (src, _) in enumerate(items)]
    to_near = [weight_copy(NEAR, i, src, tp, near) for i, (src, _) in enumerate(items)]
    onward = [weight_copy(ONWARD, i, dst(far), far, near) for i, (_, dst) in enumerate(items)]
    in_x = [weight_copy(OVER, i, dst(far), far, far) for i, (_, dst) in enumerate(items)]
    in_near = [weight_copy(NEAR, i, dst(near), near, near) for i, (_, dst) in enumerate(items)]
    in_onward = [weight_copy(ONWARD, i, dst(diagonal), diagonal, near) for i, (_, dst) in enumerate(items)]

    def pass_on(i):
        in_x[i].wait_recv()
        onward[i].start()

    def mix_copy(step):
        return remote(
            dense_ref, wts.at[me], m_send.at[step - 1], m_recv.at[step - 1], lax.rem(me + step, count_ep), tp
        )

    def mix_wait(step):
        source = lax.rem(me + count_ep - step, count_ep)
        remote(dense_ref, wts.at[source], m_send.at[step - 1], m_recv.at[step - 1], source, tp).wait_recv()

    def row_copy(link, s, piece, arrival=False):
        block, q = piece
        ref = xs.at[block, pl.ds(q * piece_rows, piece_rows)]
        known = link if arrival else far_link[link]
        return remote(ref, ref, d_send.at[link, s], d_recv.at[known, s], links[link], tp)

    order = [pick(block_of(*ORDER[END][k]), block_of(*ORDER[MID][k])) for k in range(count_ep)]

    def ordered(k):
        block = order[0]
        for i in range(1, count_ep):
            block = jnp.where(k == i, order[i], block)
        return block

    def gate_up(first, last, sources):
        def body(i, carry):
            block = ordered(first + i // (len(sources) // 2))
            for n in (0, 1):
                source = sources[n]
                if len(sources) > 2:
                    source = jnp.where(i % 2 == 1, sources[2 + n], source)
                x = xs[block]
                gate = jnp.dot(x, wg[source], preferred_element_type=jnp.float32)
                up = jnp.dot(x, wu[source], preferred_element_type=jnp.float32)
                hidden = gate / (1.0 + jnp.exp(-gate)) * up
                hid[block, :, pl.ds(pl.multiple_of(source * part, part), part)] = hidden.astype(jnp.bfloat16)
            return carry

        lax.fori_loop(0, (last - first) * (len(sources) // 2), body, 0)

    def dispatch_sends(s):
        for link in (INW, OUTW, PAIR):
            for_kinds(at(SENDS, link, s), lambda a, b: row_copy(link, s, place(a, b)).start())

    def dispatch_waits(s):
        for link in (INW, OUTW, PAIR):
            for_kinds(at(RECVS, link, s), lambda a, b: row_copy(link, s, place(a, b), True).wait_recv())

    def down(block, q):
        value = jnp.dot(
            hid[block], wd[q].reshape(count_tp * part, quarter), preferred_element_type=jnp.float32
        )
        share = jnp.concatenate([wcol[block]] * (quarter // 128), axis=1)
        return jnp.where(share > 0.0, share * value, 0.0)

    def back_copy(link, s):
        return remote(
            rout.at[link * BACK + s], rin.at[far_link[link] * BACK + s],
            r_send.at[link, s], r_recv.at[far_link[link], s], links[link], tp,
        )

    def back_wait(link, s):
        here = rin.at[link * BACK + s]
        remote(here, here, r_send.at[link, s], r_recv.at[link, s], links[link], tp).wait_recv()

    def wait_children(kids):
        shared = [c for c in kids.get(END, []) if len(kids) == 1 or c in kids.get(MID, [])]
        if len(kids) == 1:
            shared = next(iter(kids.values()))
        for c in shared:
            back_wait(*c)
        for kind, cond in ((END, is_end), (MID, is_mid)):
            extra = [c for c in kids.get(kind, []) if c not in shared]
            if extra:
                def waits(extra=extra):
                    for c in extra:
                        back_wait(*c)

                pl.when(cond)(waits)

    def arrived(kids):
        indices = []
        for n in range(max(len(v) for v in kids.values())):
            ids = [v[n][0] * BACK + v[n][1] if n < len(v) else none for v in kids.values()]
            indices.append(ids[0] if len(set(ids)) == 1 else pick(*ids))
        return indices

    def total_of(table):
        kids = {k: children(k, p) for k, p in table.items()}
        values = list(table.values())
        own = down(*place(values[0], values[-1]))
        wait_children(kids)
        total = own
        for index in arrived(kids):
            total = total + rin[index].astype(jnp.float32)
        return total

    def back_slot(link, s):
        table = at(BACK_SENDS, link, s)

        def body(*_):
            rout[link * BACK + s] = total_of(table).astype(jnp.bfloat16)
            back_copy(link, s).start()

        for_kinds(table, body)

    def ready(q):
        i = DOWN[q]
        in_near[i].wait_recv()
        in_onward[i].wait_recv()

    def final_copy(q, step):
        target = lax.rem(tp + step, count_tp)
        return remote(
            fin.at[q, target], landed.at[tp, q], f_send.at[q, step - 1], f_recv.at[q, step - 1], me, target
        )

    def final_wait(q, step):
        here = landed.at[lax.rem(tp + count_tp - step, count_tp), q]
        remote(here, here, f_send.at[q, step - 1], f_recv.at[q, step - 1], me, tp).wait_recv()

    def finish(q):
        total = total_of({END: ("O", 0, q), MID: ("O", 1, q)})
        mixed = total.astype(jnp.bfloat16)
        for c in range(count_tp):
            fin[q, c] = mixed[:, c * sub:(c + 1) * sub]
        for step in range(1, count_tp):
            final_copy(q, step).start()
        square = total * total
        lanes = squares.shape[1]
        squares[...] += sum(square[:, i:i + lanes] for i in range(0, quarter, lanes))

    chip, other_chip = (tp, near), (far, diagonal)
    everyone = chip + other_chip
    links_back = (PAIR, INW, OUTW)

    for g in range(BACK_START + BACK + 2):
        if 2 <= g < SLOTS + 2:
            dispatch_waits(g - 2)
        if g == 0:
            over_x[GATE].start()
        if g < SLOTS:
            dispatch_sends(g)
        if g == 0:
            for copy in (over_x[UP], to_near[GATE], to_near[UP]):
                copy.start()
            lax.fori_loop(piece_rows // group, rows // group, norm, 0)
        if g == 1:
            expert = lax.broadcasted_iota(jnp.int32, (wts.shape[1], ids_ref.shape[1]), 0)
            tally = jnp.sum(scores_ref[...], axis=0, keepdims=True)
            dense = jnp.zeros(expert.shape, jnp.float32)
            for k in range(ids_ref.shape[0]):
                mix = scores_ref[k:k + 1, :] / tally
                dense = dense + jnp.where(ids_ref[k:k + 1, :] == expert, mix, 0.0)
            lanes = wts.shape[2]
            dense = jnp.concatenate([dense, jnp.zeros((dense.shape[0], lanes), jnp.float32)], axis=1)
            mine_only = dense[:, :lanes]
            for k in range(1, count_tp):
                mine_only = jnp.where(tp == k, dense[:, k * rows:k * rows + lanes], mine_only)
            dense_ref[...] = mine_only
            wts[me] = mine_only
            for step in range(1, count_ep):
                mix_copy(step).start()
            for copy in mine_down:
                copy.wait()
            for q in reversed(range(QUARTERS)):
                over_x[DOWN[q]].start()
                to_near[DOWN[q]].start()
            for i in (GATE, UP):
                mine[i].wait()
                in_near[i].wait_recv()
            gate_up(0, 1, chip)
        if g == 5:
            gate_up(1, 2, chip)
        if g == 6:
            rin[none] = jnp.zeros(rin.shape[1:], rin.dtype)
            squares[...] = jnp.zeros_like(squares)
        if g == 7:
            gate_up(2, 3, chip)
            pass_on(GATE)
        if g == 8:
            for step in range(1, count_ep):
                mix_wait(step)
            for block in range(count_ep):
                turned = jnp.transpose(wts[block])
                lane = lax.broadcasted_iota(jnp.int32, turned.shape, 1)
                column = jnp.sum(jnp.where(lane == me, turned, 0.0), axis=1, keepdims=True)
                wcol[block] = jnp.broadcast_to(column[:rows], (rows, 128))
        if g == 9:
            gate_up(3, 4, chip)
        if g == 11:
            gate_up(4, 5, chip)
        if g == 12:
            pass_on(UP)
            in_onward[GATE].wait_recv()
            in_onward[UP].wait_recv()
            gate_up(3, 4, other_chip)
            gate_up(2, 3, other_chip)
        if g < BACK_START:
            continue
        r = g - BACK_START
        if r == 0:
            pass_on(DOWN[3])
            ready(3)
            back_slot(PAIR, 0)
            gate_up(5, 6, everyone)
            back_slot(INW, 0)
            back_slot(OUTW, 0)
            continue
        if r == 1:
            gate_up(6, 7, everyone)
            back_slot(PAIR, 1)
            pass_on(DOWN[2])
            ready(2)
            back_slot(INW, 1)
            back_slot(OUTW, 1)
            gate_up(4, 5, other_chip)
            continue
        if r == 4:
            ready(1)
        if r == 5:
            ready(0)
        if r < BACK:
            for link in links_back:
                back_slot(link, r)
        if r == 2:
            gate_up(0, 2, other_chip)
            pass_on(DOWN[1])
        if r == 3:
            gate_up(7, 8, everyone)
        if r == 4:
            pass_on(DOWN[0])
        if r >= BACK - 2:
            finish(BACK + 1 - r)

    mean = jnp.sum(squares[...], axis=1, keepdims=True) / width
    scale = lax.rsqrt(mean + epsilon)
    scales[tp, :, :rows] = jnp.transpose(jnp.broadcast_to(scale, squares.shape))[:scales.shape[1], :]

    def scale_copy(step):
        target = lax.rem(tp + step, count_tp)
        return remote(scales.at[tp], scales.at[tp], s_send.at[step - 1], s_recv.at[step - 1], me, target)

    def scale_wait(step):
        here = scales.at[lax.rem(tp + count_tp - step, count_tp)]
        remote(here, here, s_send.at[step - 1], s_recv.at[step - 1], me, tp).wait_recv()

    for step in range(1, count_tp):
        scale_copy(step).start()

    def result(source):
        return pltpu.make_async_copy(stage.at[source], out_ref.at[source], local_sem.at[source])

    for step in range(count_tp):
        source = lax.rem(tp + count_tp - step, count_tp)
        if step == 0:
            for q in range(QUARTERS):
                landed[tp, q] = fin[q, tp]
            column = scale
        else:
            scale_wait(step)
            column = jnp.transpose(scales[source])[:rows, :1]
            for q in range(QUARTERS):
                final_wait(q, step)
        for q in range(QUARTERS):
            at_columns = slice(q * sub, (q + 1) * sub)
            mixed = landed[source, q].astype(jnp.float32) * column * out_gain_ref[:, at_columns]
            stage[source, :, at_columns] = mixed.astype(jnp.bfloat16)
        result(source).start()

    for link in (INW, OUTW, PAIR):
        for s in range(SLOTS):
            for_kinds(at(SENDS, link, s), lambda a, b: row_copy(link, s, place(a, b)).wait_send())
        for s in range(BACK):
            for_kinds(at(BACK_SENDS, link, s), lambda a, b: back_copy(link, s).wait_send())
    for copies in (over_x, to_near, onward):
        for copy in copies:
            copy.wait_send()
    for step in range(1, count_ep):
        mix_copy(step).wait_send()
    for step in range(1, count_tp):
        scale_copy(step).wait_send()
        for q in range(QUARTERS):
            final_copy(q, step).wait_send()
    for source in range(count_tp):
        result(source).wait()


def fused(tokens, in_gain, route_ids, route_scores, gate_weight, up_weight, down_weight, out_gain):
    count_ep, count_tp = lax.axis_size("ep"), lax.axis_size("tp")
    experts = count_ep * gate_weight.shape[0]
    tok_count, width = tokens.shape
    rows = tok_count // count_tp
    part = gate_weight.shape[2]
    quarter = width // QUARTERS
    lanes = -(-rows // 128) * 128
    bf16, f32 = jnp.bfloat16, jnp.float32
    dma = pltpu.SemaphoreType.DMA
    any_space = pl.BlockSpec(memory_space=pltpu.HBM)
    in_vmem = pl.BlockSpec(memory_space=pltpu.VMEM)
    weights = 2 + QUARTERS
    sub = width // count_tp // QUARTERS
    out = pl.pallas_call(
        fused_kernel,
        name="experts",
        out_shape=jax.ShapeDtypeStruct((count_tp, rows, width // count_tp), bf16),
        in_specs=[any_space] + [in_vmem] * 4 + [any_space] * 3,
        out_specs=any_space,
        scratch_shapes=[
            pltpu.VMEM((rows, width), bf16),
            pltpu.VMEM((count_ep, rows, width), bf16),
            pltpu.VMEM((count_tp, width, part), bf16),
            pltpu.VMEM((count_tp, width, part), bf16),
            pltpu.VMEM((QUARTERS, count_tp, part, quarter), bf16),
            pltpu.VMEM((count_ep, rows, part * count_tp), bf16),
            pltpu.VMEM((3 * BACK + 1, rows, quarter), bf16),
            pltpu.VMEM((3 * BACK, rows, quarter), bf16),
            pltpu.VMEM((QUARTERS, count_tp, rows, sub), bf16),
            pltpu.VMEM((count_tp, QUARTERS, rows, sub), bf16),
            pltpu.VMEM((count_tp, rows, width // count_tp), bf16),
            pltpu.VMEM((rows, 128), f32),
            pltpu.VMEM((count_tp, 8, lanes), f32),
            pltpu.VMEM((experts, lanes), f32),
            pltpu.VMEM((count_ep, experts, lanes), f32),
            pltpu.VMEM((count_ep, rows, 128), f32),
            dma((3 + QUARTERS * count_tp,)),
            dma((3, weights)),
            dma((3, weights)),
            dma((count_ep - 1,)),
            dma((count_ep - 1,)),
            dma((3, SLOTS)),
            dma((3, SLOTS)),
            dma((3, BACK)),
            dma((3, BACK)),
            dma((QUARTERS, count_tp - 1)),
            dma((QUARTERS, count_tp - 1)),
            dma((count_tp - 1,)),
            dma((count_tp - 1,)),
        ],
        compiler_params=pltpu.CompilerParams(
            collective_id=0, has_side_effects=True, vmem_limit_bytes=63 * 2**20
        ),
    )(
        tokens, in_gain.reshape(1, width), route_ids.T, route_scores.T, out_gain.reshape(1, -1),
        gate_weight[0], up_weight[0], down_weight[0],
    )
    return out.reshape(tok_count, width // count_tp)


def solution(mesh):
    in_specs = (
        P("ep", None),
        P(),
        P("ep", None),
        P("ep", None),
        P("ep", None, "tp"),
        P("ep", None, "tp"),
        P("ep", "tp", None),
        P("tp"),
    )
    out_specs = P("ep", "tp")
    small = mesh.shape["ep"] == 2 * LINE and mesh.shape["tp"] == QUARTERS
    return jax.shard_map(
        fused if small else per_device, mesh=mesh, in_specs=in_specs, out_specs=out_specs, check_vma=False
    )
```

```python
import functools

import jax
import jax.numpy as jnp
from jax import lax
from jax.experimental import pallas as pl
from jax.experimental.pallas import tpu as pltpu
from jax.sharding import PartitionSpec as P

epsilon = 1e-06
MESH = pl.DeviceIdType.MESH


def gathered(block, count):
    blocks = [block]
    bit = 1
    swaps = []
    while bit < count:
        swaps.append([(i, i ^ bit) for i in range(count)])
        bit *= 2
    first = lax.ppermute(block, "tp", swaps[0])
    blocks.append(first)
    for pairs in swaps[1:]:
        far = lax.ppermute(block, "tp", pairs)
        blocks.append(far)
        blocks.append(lax.ppermute(far, "tp", swaps[0]))
    return blocks


def per_device(
    tokens, in_gain, route_ids, route_scores, gate_weight, up_weight, down_weight, out_gain
):
    count_ep = lax.axis_size("ep")
    count_tp = lax.axis_size("tp")
    experts = count_ep * gate_weight.shape[0]
    tok_count, full_width = tokens.shape
    rows = tok_count // count_tp
    start = lax.axis_index("tp") * rows
    gates = gathered(gate_weight[0], count_tp)
    ups = gathered(up_weight[0], count_tp)
    downs = gathered(down_weight[0], count_tp)
    gain_full = lax.all_gather(out_gain, "tp", axis=0, tiled=True)

    as_float = lax.dynamic_slice_in_dim(tokens, start, rows, 0).astype(jnp.float32)
    normed = (
        as_float
        * lax.rsqrt(jnp.mean(as_float * as_float, axis=1, keepdims=True) + epsilon)
        * in_gain
    ).astype(jnp.bfloat16)
    ring = count_ep // 2
    pair_swap = [(i, i ^ 1) for i in range(count_ep)]
    ring_step = [(i, (i + 2) % count_ep) for i in range(count_ep)]
    held = [normed]
    for _ in range(1, ring):
        held.append(lax.ppermute(held[-1], "ep", ring_step))
    partner = [lax.ppermute(block, "ep", pair_swap) for block in held]

    ids = lax.dynamic_slice_in_dim(route_ids, start, rows, 0)
    scores = lax.dynamic_slice_in_dim(route_scores, start, rows, 0)
    mix = scores / jnp.sum(scores, axis=1, keepdims=True)
    chosen = ids[:, :, None] == jnp.arange(experts, dtype=jnp.int32)[None, None, :]
    dense = jnp.sum(jnp.where(chosen, mix[:, :, None], 0.0), axis=1).T
    weight = lax.all_to_all(dense, "ep", split_axis=0, concat_axis=0, tiled=True).reshape(count_ep, rows)

    gates, ups, held = lax.optimization_barrier((gates, ups, held))
    gate_full = jnp.concatenate(gates, 1)
    up_full = jnp.concatenate(ups, 1)
    down_full = jnp.concatenate(downs, 0)
    me = lax.axis_index("ep")

    def terms_of(step):
        block = jnp.concatenate([held[step], partner[step]], 0)
        gate_acts = jnp.dot(block, gate_full, preferred_element_type=jnp.float32)
        up_acts = jnp.dot(block, up_full, preferred_element_type=jnp.float32)
        hidden = (jax.nn.silu(gate_acts) * up_acts).astype(jnp.bfloat16)
        expert_out = jnp.dot(hidden, down_full, preferred_element_type=jnp.float32)
        source = (me + count_ep - 2 * step) % count_ep
        share = jnp.concatenate(
            [
                lax.dynamic_index_in_dim(weight, source, 0, keepdims=False),
                lax.dynamic_index_in_dim(weight, source ^ 1, 0, keepdims=False),
            ]
        )[:, None]
        terms = jnp.where(share > 0.0, share * expert_out, 0.0).astype(jnp.bfloat16)
        return terms[:rows], terms[rows:]

    running = None
    for step in list(range(1, ring)) + [0]:
        own, other = terms_of(step)
        total = own.astype(jnp.float32) + lax.ppermute(other, "ep", pair_swap).astype(jnp.float32)
        if running is not None:
            total = total + lax.ppermute(running, "ep", ring_step).astype(jnp.float32)
        running = total.astype(jnp.bfloat16)
    combined = total
    scale = lax.rsqrt(jnp.mean(combined * combined, axis=1, keepdims=True) + epsilon)
    mixed = (combined * scale * gain_full).astype(jnp.bfloat16)
    return lax.all_to_all(mixed, "tp", split_axis=1, concat_axis=0, tiled=True)


END, MID = 0, 1
INW, OUTW, PAIR = 0, 1, 2
LINE = 4
QUARTERS = 4
SLOTS = 15
BACK = 14
BACK_START = 13


def seen_from_far(sends):
    other = {"O": "P", "P": "O"}
    cross = lambda p: (other[p[0]], p[1], p[2])
    mirror = lambda p: (p[0], LINE - 1 - p[1], p[2])
    return {
        (END, INW): dict(sends[MID, OUTW]),
        (END, OUTW): {},
        (END, PAIR): {s: cross(p) for s, p in sends[END, PAIR].items()},
        (MID, INW): {s: mirror(p) for s, p in sends[MID, INW].items()},
        (MID, OUTW): dict(sends[END, INW]),
        (MID, PAIR): {s: cross(p) for s, p in sends[MID, PAIR].items()},
    }


def pieces(first, *names):
    return {first + i: (n[0], int(n[1]), int(n[2])) for i, n in enumerate(names)}


FOUR = range(QUARTERS)
SENDS = {
    (END, INW): pieces(0, *(f"O0{q}" for q in FOUR), *(f"P0{q}" for q in FOUR)),
    (END, OUTW): {},
    (END, PAIR): pieces(0, *(f"O{b}{q}" for b in (0, 2, 3) for q in FOUR), "O10"),
    (MID, INW): pieces(0, *(f"O{b}{q}" for b in (1, 0) for q in FOUR)),
    (MID, OUTW): pieces(
        0, "O10", "O11", *(f"O{b}{q}" for b in (2, 3) for q in FOUR), "O12", "O13", "P11", "P12", "P13"
    ),
    (MID, PAIR): pieces(0, *(f"O{b}{q}" for b in (1, 2, 3) for q in FOUR)),
}
RECVS = seen_from_far(SENDS)
LONG = ("P23", "P33", "P32", "P22", "P31", "P30", "P21", "P20", "P11", "P10")
BACK_SENDS = {
    (END, PAIR): pieces(0, *LONG, "P03", "P02", "P01", "P00"),
    (END, INW): pieces(
        0, "O13", "O12", "O23", "O33", "O32", "O22", "O31", "O30", "O21", "O20", "P13", "P12", "O11", "O10"
    ),
    (END, OUTW): {},
    (MID, PAIR): {**pieces(0, *LONG), **pieces(12, "P13", "P12")},
    (MID, INW): pieces(4, "O23", "O33", "O32", "O22", "O31", "O30", "O21", "O20"),
    (MID, OUTW): pieces(4, "P03", "P02", "P01", "O03", "O02", "P00", "O01", "O00"),
}
BACK_RECVS = seen_from_far(BACK_SENDS)
ORDER = {
    END: [("O", 0), ("P", 0), ("O", 2), ("P", 2), ("O", 3), ("O", 1), ("P", 3), ("P", 1)],
    MID: [("O", 1), ("O", 0), ("O", 2), ("P", 2), ("O", 3), ("P", 1), ("P", 3), ("P", 0)],
}


def children(kind, piece):
    return [(l, s) for l in (INW, OUTW, PAIR) for s, p in BACK_RECVS[kind, l].items() if p == piece]


def fused_kernel(
    tok_ref, gain_in, ids_in, scores_in, out_gain_in, gate_ref, up_ref, down_ref, out_ref,
    gain_ref, ids_ref, scores_ref, out_gain_ref, tok_buf, xs, wg, wu, wd, hid, rin, rout, fin, landed, stage, squares, scales, dense_ref, wts, wcol,
    local_sem, small_sem, w_send, w_recv, m_send, m_recv, d_send, d_recv, r_send, r_recv, f_send, f_recv, s_send, s_recv,
):
    me, tp = lax.axis_index("ep"), lax.axis_index("tp")
    count_ep, rows, width = xs.shape
    count_tp = wg.shape[0]
    part = wg.shape[2]
    quarter = width // QUARTERS
    sub = width // count_tp // QUARTERS
    piece_rows = rows // QUARTERS
    none = rin.shape[0] - 1
    z, y = me // 2, me % 2
    low = z < LINE // 2
    is_end = (z == 0) | (z == LINE - 1)
    is_mid = jnp.logical_not(is_end)
    pick = lambda a, b: jnp.where(is_end, a, b)
    inward = jnp.where(low, z + 1, z - 1) * 2 + y
    outward = jnp.where(low, z - 1, z + 1) * 2 + y
    pair = z * 2 + 1 - y
    links = (inward, outward, pair)
    far_link = (pick(OUTW, INW), INW, PAIR)

    def block_of(column, b):
        line = jnp.where(low, b, LINE - 1 - b)
        return line * 2 + (y if column == "O" else 1 - y)

    def for_kinds(table, body):
        if END in table and MID in table:
            body(table[END], table[MID])
        elif END in table:
            pl.when(is_end)(lambda: body(table[END], table[END]))
        elif MID in table:
            pl.when(is_mid)(lambda: body(table[MID], table[MID]))

    def place(a, b):
        block = pick(block_of(a[0], a[1]), block_of(b[0], b[1]))
        return block, pick(a[2], b[2]) if a[2] != b[2] else a[2]

    def at(table, link, s):
        return {k: table[k, link][s] for k in (END, MID) if s in table[k, link]}

    def remote(src, dst, send, recv, ep, to):
        return pltpu.make_async_remote_copy(
            src_ref=src, dst_ref=dst, send_sem=send, recv_sem=recv, device_id=(ep, to), device_id_type=MESH
        )

    items = [(gate_ref, lambda owner: wg.at[owner]), (up_ref, lambda owner: wu.at[owner])]
    for q in reversed(range(QUARTERS)):
        items.append((wd.at[q, tp], lambda owner, q=q: wd.at[q, owner]))
    GATE, UP = 0, 1
    DOWN = {q: 2 + n for n, q in enumerate(reversed(range(QUARTERS)))}

    own_rows = pltpu.make_async_copy(tok_ref.at[pl.ds(tp * rows, rows)], tok_buf, local_sem.at[0])
    own_rows.start()
    small = [
        pltpu.make_async_copy(src, dst, small_sem.at[i])
        for i, (src, dst) in enumerate(
            ((gain_in, gain_ref), (ids_in, ids_ref), (scores_in, scores_ref), (out_gain_in, out_gain_ref))
        )
    ]
    for copy in small:
        copy.start()
    mine = [
        pltpu.make_async_copy(gate_ref, wg.at[tp], local_sem.at[1]),
        pltpu.make_async_copy(up_ref, wu.at[tp], local_sem.at[2]),
    ]
    mine_down = [
        pltpu.make_async_copy(
            down_ref.at[:, pl.ds((c * QUARTERS + q) * sub, sub)],
            wd.at[q, tp, :, pl.ds(c * sub, sub)],
            local_sem.at[3 + q * count_tp + c],
        )
        for q in range(QUARTERS)
        for c in range(count_tp)
    ]
    for copy in mine + mine_down:
        copy.start()

    barrier = pltpu.get_barrier_semaphore()
    for step in range(1, count_ep):
        pl.semaphore_signal(barrier, inc=1, device_id=(lax.rem(me + step, count_ep), tp), device_id_type=MESH)
    for step in range(1, count_tp):
        pl.semaphore_signal(barrier, inc=1, device_id=(me, lax.rem(tp + step, count_tp)), device_id_type=MESH)

    own_rows.wait()
    for copy in small:
        copy.wait()
    group = 16

    def norm(i, carry):
        at_rows = pl.ds(pl.multiple_of(i * group, group), group)
        value = tok_buf[at_rows, :].astype(jnp.float32)
        scale = lax.rsqrt(jnp.mean(value * value, axis=1, keepdims=True) + epsilon)
        xs[me, at_rows, :] = (value * scale * gain_ref[...]).astype(jnp.bfloat16)
        return carry

    lax.fori_loop(0, piece_rows // group, norm, 0)
    pl.semaphore_wait(barrier, count_ep + count_tp - 2)

    near, far = tp + 1 - 2 * (tp % 2), lax.rem(tp + 2, count_tp)
    diagonal = far + 1 - 2 * (far % 2)
    OVER, NEAR, ONWARD = 0, 1, 2

    def weight_copy(way, i, src, owner, target):
        return remote(src, items[i][1](owner), w_send.at[way, i], w_recv.at[way, i], me, target)

    over_x = [weight_copy(OVER, i, src, tp, far) for i, (src, _) in enumerate(items)]
    to_near = [weight_copy(NEAR, i, src, tp, near) for i, (src, _) in enumerate(items)]
    onward = [weight_copy(ONWARD, i, dst(far), far, near) for i, (_, dst) in enumerate(items)]
    in_x = [weight_copy(OVER, i, dst(far), far, far) for i, (_, dst) in enumerate(items)]
    in_near = [weight_copy(NEAR, i, dst(near), near, near) for i, (_, dst) in enumerate(items)]
    in_onward = [weight_copy(ONWARD, i, dst(diagonal), diagonal, near) for i, (_, dst) in enumerate(items)]

    def pass_on(i):
        in_x[i].wait_recv()
        onward[i].start()

    def mix_copy(step):
        return remote(
            dense_ref, wts.at[me], m_send.at[step - 1], m_recv.at[step - 1], lax.rem(me + step, count_ep), tp
        )

    def mix_wait(step):
        source = lax.rem(me + count_ep - step, count_ep)
        remote(dense_ref, wts.at[source], m_send.at[step - 1], m_recv.at[step - 1], source, tp).wait_recv()

    def row_copy(link, s, piece, arrival=False):
        block, q = piece
        ref = xs.at[block, pl.ds(q * piece_rows, piece_rows)]
        known = link if arrival else far_link[link]
        return remote(ref, ref, d_send.at[link, s], d_recv.at[known, s], links[link], tp)

    order = [pick(block_of(*ORDER[END][k]), block_of(*ORDER[MID][k])) for k in range(count_ep)]

    def ordered(k):
        block = order[0]
        for i in range(1, count_ep):
            block = jnp.where(k == i, order[i], block)
        return block

    def gate_up(first, last, sources):
        def body(i, carry):
            block = ordered(first + i // (len(sources) // 2))
            for n in (0, 1):
                source = sources[n]
                if len(sources) > 2:
                    source = jnp.where(i % 2 == 1, sources[2 + n], source)
                x = xs[block]
                gate = jnp.dot(x, wg[source], preferred_element_type=jnp.float32)
                up = jnp.dot(x, wu[source], preferred_element_type=jnp.float32)
                hidden = gate / (1.0 + jnp.exp(-gate)) * up
                hid[block, :, pl.ds(pl.multiple_of(source * part, part), part)] = hidden.astype(jnp.bfloat16)
            return carry

        lax.fori_loop(0, (last - first) * (len(sources) // 2), body, 0)

    def dispatch_sends(s):
        for link in (INW, OUTW, PAIR):
            for_kinds(at(SENDS, link, s), lambda a, b: row_copy(link, s, place(a, b)).start())

    def dispatch_waits(s):
        for link in (INW, OUTW, PAIR):
            for_kinds(at(RECVS, link, s), lambda a, b: row_copy(link, s, place(a, b), True).wait_recv())

    def down(block, q):
        value = jnp.dot(
            hid[block], wd[q].reshape(count_tp * part, quarter), preferred_element_type=jnp.float32
        )
        share = jnp.concatenate([wcol[block]] * (quarter // 128), axis=1)
        return jnp.where(share > 0.0, share * value, 0.0)

    def back_copy(link, s):
        return remote(
            rout.at[link * BACK + s], rin.at[far_link[link] * BACK + s],
            r_send.at[link, s], r_recv.at[far_link[link], s], links[link], tp,
        )

    def back_wait(link, s):
        here = rin.at[link * BACK + s]
        remote(here, here, r_send.at[link, s], r_recv.at[link, s], links[link], tp).wait_recv()

    def wait_children(kids):
        shared = [c for c in kids.get(END, []) if len(kids) == 1 or c in kids.get(MID, [])]
        if len(kids) == 1:
            shared = next(iter(kids.values()))
        for c in shared:
            back_wait(*c)
        for kind, cond in ((END, is_end), (MID, is_mid)):
            extra = [c for c in kids.get(kind, []) if c not in shared]
            if extra:
                def waits(extra=extra):
                    for c in extra:
                        back_wait(*c)

                pl.when(cond)(waits)

    def arrived(kids):
        indices = []
        for n in range(max(len(v) for v in kids.values())):
            ids = [v[n][0] * BACK + v[n][1] if n < len(v) else none for v in kids.values()]
            indices.append(ids[0] if len(set(ids)) == 1 else pick(*ids))
        return indices

    def total_of(table):
        kids = {k: children(k, p) for k, p in table.items()}
        values = list(table.values())
        own = down(*place(values[0], values[-1]))
        wait_children(kids)
        total = own
        for index in arrived(kids):
            total = total + rin[index].astype(jnp.float32)
        return total

    def back_slot(link, s):
        table = at(BACK_SENDS, link, s)

        def body(*_):
            rout[link * BACK + s] = total_of(table).astype(jnp.bfloat16)
            back_copy(link, s).start()

        for_kinds(table, body)

    def ready(q):
        i = DOWN[q]
        in_near[i].wait_recv()
        in_onward[i].wait_recv()

    def final_copy(q, step):
        target = lax.rem(tp + step, count_tp)
        return remote(
            fin.at[q, target], landed.at[tp, q], f_send.at[q, step - 1], f_recv.at[q, step - 1], me, target
        )

    def final_wait(q, step):
        here = landed.at[lax.rem(tp + count_tp - step, count_tp), q]
        remote(here, here, f_send.at[q, step - 1], f_recv.at[q, step - 1], me, tp).wait_recv()

    def finish(q):
        total = total_of({END: ("O", 0, q), MID: ("O", 1, q)})
        mixed = total.astype(jnp.bfloat16)
        for c in range(count_tp):
            fin[q, c] = mixed[:, c * sub:(c + 1) * sub]
        for step in range(1, count_tp):
            final_copy(q, step).start()
        square = total * total
        lanes = squares.shape[1]
        squares[...] += sum(square[:, i:i + lanes] for i in range(0, quarter, lanes))

    chip, other_chip = (tp, near), (far, diagonal)
    everyone = chip + other_chip
    links_back = (PAIR, INW, OUTW)

    for g in range(BACK_START + BACK + 2):
        if 2 <= g < SLOTS + 2:
            dispatch_waits(g - 2)
        if g == 0:
            over_x[GATE].start()
        if g < SLOTS:
            dispatch_sends(g)
        if g == 0:
            for copy in (over_x[UP], to_near[GATE], to_near[UP]):
                copy.start()
            lax.fori_loop(piece_rows // group, rows // group, norm, 0)
        if g == 1:
            expert = lax.broadcasted_iota(jnp.int32, (wts.shape[1], ids_ref.shape[1]), 0)
            tally = jnp.sum(scores_ref[...], axis=0, keepdims=True)
            dense = jnp.zeros(expert.shape, jnp.float32)
            for k in range(ids_ref.shape[0]):
                mix = scores_ref[k:k + 1, :] / tally
                dense = dense + jnp.where(ids_ref[k:k + 1, :] == expert, mix, 0.0)
            lanes = wts.shape[2]
            dense = jnp.concatenate([dense, jnp.zeros((dense.shape[0], lanes), jnp.float32)], axis=1)
            mine_only = dense[:, :lanes]
            for k in range(1, count_tp):
                mine_only = jnp.where(tp == k, dense[:, k * rows:k * rows + lanes], mine_only)
            dense_ref[...] = mine_only
            wts[me] = mine_only
            for step in range(1, count_ep):
                mix_copy(step).start()
            for copy in mine_down:
                copy.wait()
            for q in reversed(range(QUARTERS)):
                over_x[DOWN[q]].start()
                to_near[DOWN[q]].start()
            for i in (GATE, UP):
                mine[i].wait()
                in_near[i].wait_recv()
            gate_up(0, 1, chip)
        if g == 5:
            gate_up(1, 2, chip)
        if g == 6:
            rin[none] = jnp.zeros(rin.shape[1:], rin.dtype)
            squares[...] = jnp.zeros_like(squares)
        if g == 7:
            gate_up(2, 3, chip)
            pass_on(GATE)
        if g == 8:
            for step in range(1, count_ep):
                mix_wait(step)
            for block in range(count_ep):
                turned = jnp.transpose(wts[block])
                lane = lax.broadcasted_iota(jnp.int32, turned.shape, 1)
                column = jnp.sum(jnp.where(lane == me, turned, 0.0), axis=1, keepdims=True)
                wcol[block] = jnp.broadcast_to(column[:rows], (rows, 128))
        if g == 9:
            gate_up(3, 4, chip)
        if g == 11:
            gate_up(4, 5, chip)
        if g == 12:
            pass_on(UP)
            in_onward[GATE].wait_recv()
            in_onward[UP].wait_recv()
            gate_up(3, 4, other_chip)
            gate_up(2, 3, other_chip)
        if g < BACK_START:
            continue
        r = g - BACK_START
        if r == 0:
            pass_on(DOWN[3])
            ready(3)
            back_slot(PAIR, 0)
            gate_up(5, 6, everyone)
            back_slot(INW, 0)
            back_slot(OUTW, 0)
            continue
        if r == 1:
            gate_up(6, 7, everyone)
            back_slot(PAIR, 1)
            pass_on(DOWN[2])
            ready(2)
            back_slot(INW, 1)
            back_slot(OUTW, 1)
            gate_up(4, 5, other_chip)
            continue
        if r == 4:
            ready(1)
        if r == 5:
            ready(0)
        if r < BACK:
            for link in links_back:
                back_slot(link, r)
        if r == 2:
            gate_up(0, 2, other_chip)
            pass_on(DOWN[1])
        if r == 3:
            gate_up(7, 8, everyone)
        if r == 4:
            pass_on(DOWN[0])
        if r >= BACK - 2:
            finish(BACK + 1 - r)

    mean = jnp.sum(squares[...], axis=1, keepdims=True) / width
    scale = lax.rsqrt(mean + epsilon)
    scales[tp, :, :rows] = jnp.transpose(jnp.broadcast_to(scale, squares.shape))[:scales.shape[1], :]

    def scale_copy(step):
        target = lax.rem(tp + step, count_tp)
        return remote(scales.at[tp], scales.at[tp], s_send.at[step - 1], s_recv.at[step - 1], me, target)

    def scale_wait(step):
        here = scales.at[lax.rem(tp + count_tp - step, count_tp)]
        remote(here, here, s_send.at[step - 1], s_recv.at[step - 1], me, tp).wait_recv()

    for step in range(1, count_tp):
        scale_copy(step).start()

    def result(source):
        return pltpu.make_async_copy(stage.at[source], out_ref.at[source], local_sem.at[source])

    for step in range(count_tp):
        source = lax.rem(tp + count_tp - step, count_tp)
        if step == 0:
            for q in range(QUARTERS):
                landed[tp, q] = fin[q, tp]
            column = scale
        else:
            scale_wait(step)
            column = jnp.transpose(scales[source])[:rows, :1]
            for q in range(QUARTERS):
                final_wait(q, step)
        for q in range(QUARTERS):
            at_columns = slice(q * sub, (q + 1) * sub)
            mixed = landed[source, q].astype(jnp.float32) * column * out_gain_ref[:, at_columns]
            stage[source, :, at_columns] = mixed.astype(jnp.bfloat16)
        result(source).start()

    for link in (INW, OUTW, PAIR):
        for s in range(SLOTS):
            for_kinds(at(SENDS, link, s), lambda a, b: row_copy(link, s, place(a, b)).wait_send())
        for s in range(BACK):
            for_kinds(at(BACK_SENDS, link, s), lambda a, b: back_copy(link, s).wait_send())
    for copies in (over_x, to_near, onward):
        for copy in copies:
            copy.wait_send()
    for step in range(1, count_ep):
        mix_copy(step).wait_send()
    for step in range(1, count_tp):
        scale_copy(step).wait_send()
        for q in range(QUARTERS):
            final_copy(q, step).wait_send()
    for source in range(count_tp):
        result(source).wait()


def fused(tokens, in_gain, route_ids, route_scores, gate_weight, up_weight, down_weight, out_gain):
    count_ep, count_tp = lax.axis_size("ep"), lax.axis_size("tp")
    experts = count_ep * gate_weight.shape[0]
    tok_count, width = tokens.shape
    rows = tok_count // count_tp
    part = gate_weight.shape[2]
    quarter = width // QUARTERS
    lanes = -(-rows // 128) * 128
    bf16, f32 = jnp.bfloat16, jnp.float32
    dma = pltpu.SemaphoreType.DMA
    any_space = pl.BlockSpec(memory_space=pltpu.HBM)
    weights = 2 + QUARTERS
    sub = width // count_tp // QUARTERS
    out = pl.pallas_call(
        fused_kernel,
        name="experts",
        out_shape=jax.ShapeDtypeStruct((count_tp, rows, width // count_tp), bf16),
        in_specs=[any_space] * 8,
        out_specs=any_space,
        scratch_shapes=[
            pltpu.VMEM((1, width), f32),
            pltpu.VMEM(route_ids.T.shape, route_ids.dtype),
            pltpu.VMEM(route_scores.T.shape, f32),
            pltpu.VMEM((1, width // count_tp), f32),
            pltpu.VMEM((rows, width), bf16),
            pltpu.VMEM((count_ep, rows, width), bf16),
            pltpu.VMEM((count_tp, width, part), bf16),
            pltpu.VMEM((count_tp, width, part), bf16),
            pltpu.VMEM((QUARTERS, count_tp, part, quarter), bf16),
            pltpu.VMEM((count_ep, rows, part * count_tp), bf16),
            pltpu.VMEM((3 * BACK + 1, rows, quarter), bf16),
            pltpu.VMEM((3 * BACK, rows, quarter), bf16),
            pltpu.VMEM((QUARTERS, count_tp, rows, sub), bf16),
            pltpu.VMEM((count_tp, QUARTERS, rows, sub), bf16),
            pltpu.VMEM((count_tp, rows, width // count_tp), bf16),
            pltpu.VMEM((rows, 128), f32),
            pltpu.VMEM((count_tp, 8, lanes), f32),
            pltpu.VMEM((experts, lanes), f32),
            pltpu.VMEM((count_ep, experts, lanes), f32),
            pltpu.VMEM((count_ep, rows, 128), f32),
            dma((3 + QUARTERS * count_tp,)),
            dma((4,)),
            dma((3, weights)),
            dma((3, weights)),
            dma((count_ep - 1,)),
            dma((count_ep - 1,)),
            dma((3, SLOTS)),
            dma((3, SLOTS)),
            dma((3, BACK)),
            dma((3, BACK)),
            dma((QUARTERS, count_tp - 1)),
            dma((QUARTERS, count_tp - 1)),
            dma((count_tp - 1,)),
            dma((count_tp - 1,)),
        ],
        compiler_params=pltpu.CompilerParams(
            collective_id=0, has_side_effects=True, vmem_limit_bytes=63 * 2**20
        ),
    )(
        tokens, in_gain.reshape(1, width), route_ids.T, route_scores.T, out_gain.reshape(1, -1),
        gate_weight[0], up_weight[0], down_weight[0],
    )
    return out.reshape(tok_count, width // count_tp)


def solution(mesh):
    in_specs = (
        P("ep", None),
        P(),
        P("ep", None),
        P("ep", None),
        P("ep", None, "tp"),
        P("ep", None, "tp"),
        P("ep", "tp", None),
        P("tp"),
    )
    out_specs = P("ep", "tp")
    small = mesh.shape["ep"] == 2 * LINE and mesh.shape["tp"] == QUARTERS
    return jax.shard_map(
        fused if small else per_device, mesh=mesh, in_specs=in_specs, out_specs=out_specs, check_vma=False
    )
```

```python
import functools

import jax
import jax.numpy as jnp
from jax import lax
from jax.experimental import pallas as pl
from jax.experimental.pallas import tpu as pltpu
from jax.sharding import PartitionSpec as P

epsilon = 1e-06
MESH = pl.DeviceIdType.MESH


def gathered(block, count):
    blocks = [block]
    bit = 1
    swaps = []
    while bit < count:
        swaps.append([(i, i ^ bit) for i in range(count)])
        bit *= 2
    first = lax.ppermute(block, "tp", swaps[0])
    blocks.append(first)
    for pairs in swaps[1:]:
        far = lax.ppermute(block, "tp", pairs)
        blocks.append(far)
        blocks.append(lax.ppermute(far, "tp", swaps[0]))
    return blocks


def per_device(
    tokens, in_gain, route_ids, route_scores, gate_weight, up_weight, down_weight, out_gain
):
    count_ep = lax.axis_size("ep")
    count_tp = lax.axis_size("tp")
    experts = count_ep * gate_weight.shape[0]
    tok_count, full_width = tokens.shape
    rows = tok_count // count_tp
    start = lax.axis_index("tp") * rows
    gates = gathered(gate_weight[0], count_tp)
    ups = gathered(up_weight[0], count_tp)
    downs = gathered(down_weight[0], count_tp)
    gain_full = lax.all_gather(out_gain, "tp", axis=0, tiled=True)

    as_float = lax.dynamic_slice_in_dim(tokens, start, rows, 0).astype(jnp.float32)
    normed = (
        as_float
        * lax.rsqrt(jnp.mean(as_float * as_float, axis=1, keepdims=True) + epsilon)
        * in_gain
    ).astype(jnp.bfloat16)
    ring = count_ep // 2
    pair_swap = [(i, i ^ 1) for i in range(count_ep)]
    ring_step = [(i, (i + 2) % count_ep) for i in range(count_ep)]
    held = [normed]
    for _ in range(1, ring):
        held.append(lax.ppermute(held[-1], "ep", ring_step))
    partner = [lax.ppermute(block, "ep", pair_swap) for block in held]

    ids = lax.dynamic_slice_in_dim(route_ids, start, rows, 0)
    scores = lax.dynamic_slice_in_dim(route_scores, start, rows, 0)
    mix = scores / jnp.sum(scores, axis=1, keepdims=True)
    chosen = ids[:, :, None] == jnp.arange(experts, dtype=jnp.int32)[None, None, :]
    dense = jnp.sum(jnp.where(chosen, mix[:, :, None], 0.0), axis=1).T
    weight = lax.all_to_all(dense, "ep", split_axis=0, concat_axis=0, tiled=True).reshape(count_ep, rows)

    gates, ups, held = lax.optimization_barrier((gates, ups, held))
    gate_full = jnp.concatenate(gates, 1)
    up_full = jnp.concatenate(ups, 1)
    down_full = jnp.concatenate(downs, 0)
    me = lax.axis_index("ep")

    def terms_of(step):
        block = jnp.concatenate([held[step], partner[step]], 0)
        gate_acts = jnp.dot(block, gate_full, preferred_element_type=jnp.float32)
        up_acts = jnp.dot(block, up_full, preferred_element_type=jnp.float32)
        hidden = (jax.nn.silu(gate_acts) * up_acts).astype(jnp.bfloat16)
        expert_out = jnp.dot(hidden, down_full, preferred_element_type=jnp.float32)
        source = (me + count_ep - 2 * step) % count_ep
        share = jnp.concatenate(
            [
                lax.dynamic_index_in_dim(weight, source, 0, keepdims=False),
                lax.dynamic_index_in_dim(weight, source ^ 1, 0, keepdims=False),
            ]
        )[:, None]
        terms = jnp.where(share > 0.0, share * expert_out, 0.0).astype(jnp.bfloat16)
        return terms[:rows], terms[rows:]

    running = None
    for step in list(range(1, ring)) + [0]:
        own, other = terms_of(step)
        total = own.astype(jnp.float32) + lax.ppermute(other, "ep", pair_swap).astype(jnp.float32)
        if running is not None:
            total = total + lax.ppermute(running, "ep", ring_step).astype(jnp.float32)
        running = total.astype(jnp.bfloat16)
    combined = total
    scale = lax.rsqrt(jnp.mean(combined * combined, axis=1, keepdims=True) + epsilon)
    mixed = (combined * scale * gain_full).astype(jnp.bfloat16)
    return lax.all_to_all(mixed, "tp", split_axis=1, concat_axis=0, tiled=True)


END, MID = 0, 1
INW, OUTW, PAIR = 0, 1, 2
LINE = 4
QUARTERS = 4
SLOTS = 15
BACK = 14
BACK_START = 13


def seen_from_far(sends):
    other = {"O": "P", "P": "O"}
    cross = lambda p: (other[p[0]], p[1], p[2])
    mirror = lambda p: (p[0], LINE - 1 - p[1], p[2])
    return {
        (END, INW): dict(sends[MID, OUTW]),
        (END, OUTW): {},
        (END, PAIR): {s: cross(p) for s, p in sends[END, PAIR].items()},
        (MID, INW): {s: mirror(p) for s, p in sends[MID, INW].items()},
        (MID, OUTW): dict(sends[END, INW]),
        (MID, PAIR): {s: cross(p) for s, p in sends[MID, PAIR].items()},
    }


def pieces(first, *names):
    return {first + i: (n[0], int(n[1]), int(n[2])) for i, n in enumerate(names)}


FOUR = range(QUARTERS)
SENDS = {
    (END, INW): pieces(0, *(f"O0{q}" for q in FOUR), *(f"P0{q}" for q in FOUR)),
    (END, OUTW): {},
    (END, PAIR): pieces(0, *(f"O{b}{q}" for b in (0, 2, 3) for q in FOUR), "O10"),
    (MID, INW): pieces(0, *(f"O{b}{q}" for b in (1, 0) for q in FOUR)),
    (MID, OUTW): pieces(
        0, "O10", "O11", *(f"O{b}{q}" for b in (2, 3) for q in FOUR), "O12", "O13", "P11", "P12", "P13"
    ),
    (MID, PAIR): pieces(0, *(f"O{b}{q}" for b in (1, 2, 3) for q in FOUR)),
}
RECVS = seen_from_far(SENDS)
LONG = ("P23", "P33", "P32", "P22", "P31", "P30", "P21", "P20", "P11", "P10")
BACK_SENDS = {
    (END, PAIR): pieces(0, *LONG, "P03", "P02", "P01", "P00"),
    (END, INW): pieces(
        0, "O13", "O12", "O23", "O33", "O32", "O22", "O31", "O30", "O21", "O20", "P13", "P12", "O11", "O10"
    ),
    (END, OUTW): {},
    (MID, PAIR): {**pieces(0, *LONG), **pieces(12, "P13", "P12")},
    (MID, INW): pieces(4, "O23", "O33", "O32", "O22", "O31", "O30", "O21", "O20"),
    (MID, OUTW): pieces(4, "P03", "P02", "P01", "O03", "O02", "P00", "O01", "O00"),
}
BACK_RECVS = seen_from_far(BACK_SENDS)
ORDER = {
    END: [("O", 0), ("P", 0), ("O", 2), ("P", 2), ("O", 3), ("O", 1), ("P", 3), ("P", 1)],
    MID: [("O", 1), ("O", 0), ("O", 2), ("P", 2), ("O", 3), ("P", 1), ("P", 3), ("P", 0)],
}


def children(kind, piece):
    return [(l, s) for l in (INW, OUTW, PAIR) for s, p in BACK_RECVS[kind, l].items() if p == piece]


def fused_kernel(
    tok_ref, gain_in, ids_in, scores_in, out_gain_in, gate_ref, up_ref, down_ref, out_ref,
    gain_ref, ids_ref, scores_ref, out_gain_ref, tok_buf, xs, wg, wu, wd, hid, rin, rout, fin, landed, stage, squares, scales, dense_ref, wts, wcol,
    local_sem, small_sem, w_send, w_recv, m_send, m_recv, d_send, d_recv, r_send, r_recv, f_send, f_recv, s_send, s_recv,
):
    me, tp = lax.axis_index("ep"), lax.axis_index("tp")
    count_ep, rows, width = xs.shape
    count_tp = wg.shape[0]
    part = wg.shape[2]
    quarter = width // QUARTERS
    sub = width // count_tp // QUARTERS
    piece_rows = rows // QUARTERS
    none = rin.shape[0] - 1
    z, y = me // 2, me % 2
    low = z < LINE // 2
    is_end = (z == 0) | (z == LINE - 1)
    is_mid = jnp.logical_not(is_end)
    pick = lambda a, b: jnp.where(is_end, a, b)
    inward = jnp.where(low, z + 1, z - 1) * 2 + y
    outward = jnp.where(low, z - 1, z + 1) * 2 + y
    pair = z * 2 + 1 - y
    links = (inward, outward, pair)
    far_link = (pick(OUTW, INW), INW, PAIR)

    def block_of(column, b):
        line = jnp.where(low, b, LINE - 1 - b)
        return line * 2 + (y if column == "O" else 1 - y)

    def for_kinds(table, body):
        if END in table and MID in table:
            body(table[END], table[MID])
        elif END in table:
            pl.when(is_end)(lambda: body(table[END], table[END]))
        elif MID in table:
            pl.when(is_mid)(lambda: body(table[MID], table[MID]))

    def place(a, b):
        block = pick(block_of(a[0], a[1]), block_of(b[0], b[1]))
        return block, pick(a[2], b[2]) if a[2] != b[2] else a[2]

    def at(table, link, s):
        return {k: table[k, link][s] for k in (END, MID) if s in table[k, link]}

    def remote(src, dst, send, recv, ep, to):
        return pltpu.make_async_remote_copy(
            src_ref=src, dst_ref=dst, send_sem=send, recv_sem=recv, device_id=(ep, to), device_id_type=MESH
        )

    items = [(gate_ref, lambda owner: wg.at[owner])]
    half = width // 2
    for h in range(2):
        at_half = pl.ds(h * half, half)
        items.append((up_ref.at[at_half], lambda owner, at_half=at_half: wu.at[owner, at_half]))
    for q in reversed(range(QUARTERS)):
        items.append((wd.at[q, tp], lambda owner, q=q: wd.at[q, owner]))
    GATE, UP, UP_END = 0, 1, 2
    DOWN = {q: 3 + n for n, q in enumerate(reversed(range(QUARTERS)))}

    own_rows = pltpu.make_async_copy(tok_ref.at[pl.ds(tp * rows, rows)], tok_buf, local_sem.at[0])
    own_rows.start()
    small = [
        pltpu.make_async_copy(src, dst, small_sem.at[i])
        for i, (src, dst) in enumerate(
            ((gain_in, gain_ref), (ids_in, ids_ref), (scores_in, scores_ref), (out_gain_in, out_gain_ref))
        )
    ]
    for copy in small:
        copy.start()
    mine = [
        pltpu.make_async_copy(gate_ref, wg.at[tp], local_sem.at[1]),
        pltpu.make_async_copy(up_ref, wu.at[tp], local_sem.at[2]),
    ]
    mine_down = [
        pltpu.make_async_copy(
            down_ref.at[:, pl.ds((c * QUARTERS + q) * sub, sub)],
            wd.at[q, tp, :, pl.ds(c * sub, sub)],
            local_sem.at[3 + q * count_tp + c],
        )
        for q in range(QUARTERS)
        for c in range(count_tp)
    ]
    for copy in mine + mine_down:
        copy.start()

    barrier = pltpu.get_barrier_semaphore()
    for step in range(1, count_ep):
        pl.semaphore_signal(barrier, inc=1, device_id=(lax.rem(me + step, count_ep), tp), device_id_type=MESH)
    for step in range(1, count_tp):
        pl.semaphore_signal(barrier, inc=1, device_id=(me, lax.rem(tp + step, count_tp)), device_id_type=MESH)

    own_rows.wait()
    for copy in small:
        copy.wait()
    group = 16

    def norm(i, carry):
        at_rows = pl.ds(pl.multiple_of(i * group, group), group)
        value = tok_buf[at_rows, :].astype(jnp.float32)
        scale = lax.rsqrt(jnp.mean(value * value, axis=1, keepdims=True) + epsilon)
        xs[me, at_rows, :] = (value * scale * gain_ref[...]).astype(jnp.bfloat16)
        return carry

    lax.fori_loop(0, piece_rows // group, norm, 0)
    pl.semaphore_wait(barrier, count_ep + count_tp - 2)

    near, far = tp + 1 - 2 * (tp % 2), lax.rem(tp + 2, count_tp)
    diagonal = far + 1 - 2 * (far % 2)
    OVER, NEAR, ONWARD = 0, 1, 2

    def weight_copy(way, i, src, owner, target):
        return remote(src, items[i][1](owner), w_send.at[way, i], w_recv.at[way, i], me, target)

    over_x = [weight_copy(OVER, i, src, tp, far) for i, (src, _) in enumerate(items)]
    to_near = [weight_copy(NEAR, i, src, tp, near) for i, (src, _) in enumerate(items)]
    onward = [weight_copy(ONWARD, i, dst(far), far, near) for i, (_, dst) in enumerate(items)]
    in_x = [weight_copy(OVER, i, dst(far), far, far) for i, (_, dst) in enumerate(items)]
    in_near = [weight_copy(NEAR, i, dst(near), near, near) for i, (_, dst) in enumerate(items)]
    in_onward = [weight_copy(ONWARD, i, dst(diagonal), diagonal, near) for i, (_, dst) in enumerate(items)]

    def pass_on(i):
        in_x[i].wait_recv()
        onward[i].start()

    def mix_copy(step):
        return remote(
            dense_ref, wts.at[me], m_send.at[step - 1], m_recv.at[step - 1], lax.rem(me + step, count_ep), tp
        )

    def mix_wait(step):
        source = lax.rem(me + count_ep - step, count_ep)
        remote(dense_ref, wts.at[source], m_send.at[step - 1], m_recv.at[step - 1], source, tp).wait_recv()

    def row_copy(link, s, piece, arrival=False):
        block, q = piece
        ref = xs.at[block, pl.ds(q * piece_rows, piece_rows)]
        known = link if arrival else far_link[link]
        return remote(ref, ref, d_send.at[link, s], d_recv.at[known, s], links[link], tp)

    order = [pick(block_of(*ORDER[END][k]), block_of(*ORDER[MID][k])) for k in range(count_ep)]

    def ordered(k):
        block = order[0]
        for i in range(1, count_ep):
            block = jnp.where(k == i, order[i], block)
        return block

    def gate_up(first, last, sources):
        def body(i, carry):
            block = ordered(first + i // (len(sources) // 2))
            for n in (0, 1):
                source = sources[n]
                if len(sources) > 2:
                    source = jnp.where(i % 2 == 1, sources[2 + n], source)
                x = xs[block]
                gate = jnp.dot(x, wg[source], preferred_element_type=jnp.float32)
                up = jnp.dot(x, wu[source], preferred_element_type=jnp.float32)
                hidden = gate / (1.0 + jnp.exp(-gate)) * up
                hid[block, :, pl.ds(pl.multiple_of(source * part, part), part)] = hidden.astype(jnp.bfloat16)
            return carry

        lax.fori_loop(0, (last - first) * (len(sources) // 2), body, 0)

    def dispatch_sends(s):
        for link in (INW, OUTW, PAIR):
            for_kinds(at(SENDS, link, s), lambda a, b: row_copy(link, s, place(a, b)).start())

    def dispatch_waits(s):
        for link in (INW, OUTW, PAIR):
            for_kinds(at(RECVS, link, s), lambda a, b: row_copy(link, s, place(a, b), True).wait_recv())

    def down(block, q):
        value = jnp.dot(
            hid[block], wd[q].reshape(count_tp * part, quarter), preferred_element_type=jnp.float32
        )
        share = jnp.concatenate([wcol[block]] * (quarter // 128), axis=1)
        return jnp.where(share > 0.0, share * value, 0.0)

    def back_copy(link, s):
        return remote(
            rout.at[link * BACK + s], rin.at[far_link[link] * BACK + s],
            r_send.at[link, s], r_recv.at[far_link[link], s], links[link], tp,
        )

    def back_wait(link, s):
        here = rin.at[link * BACK + s]
        remote(here, here, r_send.at[link, s], r_recv.at[link, s], links[link], tp).wait_recv()

    def wait_children(kids):
        shared = [c for c in kids.get(END, []) if len(kids) == 1 or c in kids.get(MID, [])]
        if len(kids) == 1:
            shared = next(iter(kids.values()))
        for c in shared:
            back_wait(*c)
        for kind, cond in ((END, is_end), (MID, is_mid)):
            extra = [c for c in kids.get(kind, []) if c not in shared]
            if extra:
                def waits(extra=extra):
                    for c in extra:
                        back_wait(*c)

                pl.when(cond)(waits)

    def arrived(kids):
        indices = []
        for n in range(max(len(v) for v in kids.values())):
            ids = [v[n][0] * BACK + v[n][1] if n < len(v) else none for v in kids.values()]
            indices.append(ids[0] if len(set(ids)) == 1 else pick(*ids))
        return indices

    def total_of(table):
        kids = {k: children(k, p) for k, p in table.items()}
        values = list(table.values())
        own = down(*place(values[0], values[-1]))
        wait_children(kids)
        total = own
        for index in arrived(kids):
            total = total + rin[index].astype(jnp.float32)
        return total

    def back_slot(link, s):
        table = at(BACK_SENDS, link, s)

        def body(*_):
            rout[link * BACK + s] = total_of(table).astype(jnp.bfloat16)
            back_copy(link, s).start()

        for_kinds(table, body)

    def ready(q):
        i = DOWN[q]
        in_near[i].wait_recv()
        in_onward[i].wait_recv()

    def final_copy(q, step):
        target = lax.rem(tp + step, count_tp)
        return remote(
            fin.at[q, target], landed.at[tp, q], f_send.at[q, step - 1], f_recv.at[q, step - 1], me, target
        )

    def final_wait(q, step):
        here = landed.at[lax.rem(tp + count_tp - step, count_tp), q]
        remote(here, here, f_send.at[q, step - 1], f_recv.at[q, step - 1], me, tp).wait_recv()

    def finish(q):
        total = total_of({END: ("O", 0, q), MID: ("O", 1, q)})
        mixed = total.astype(jnp.bfloat16)
        for c in range(count_tp):
            fin[q, c] = mixed[:, c * sub:(c + 1) * sub]
        for step in range(1, count_tp):
            final_copy(q, step).start()
        square = total * total
        lanes = squares.shape[1]
        squares[...] += sum(square[:, i:i + lanes] for i in range(0, quarter, lanes))

    chip, other_chip = (tp, near), (far, diagonal)
    everyone = chip + other_chip
    links_back = (PAIR, INW, OUTW)

    for g in range(BACK_START + BACK + 2):
        if 2 <= g < SLOTS + 2:
            dispatch_waits(g - 2)
        if g == 0:
            over_x[GATE].start()
        if g < SLOTS:
            dispatch_sends(g)
        if g == 0:
            for copy in over_x[UP:UP_END + 1] + to_near[:UP_END + 1]:
                copy.start()
            lax.fori_loop(piece_rows // group, rows // group, norm, 0)
        if g == 1:
            expert = lax.broadcasted_iota(jnp.int32, (wts.shape[1], ids_ref.shape[1]), 0)
            tally = jnp.sum(scores_ref[...], axis=0, keepdims=True)
            dense = jnp.zeros(expert.shape, jnp.float32)
            for k in range(ids_ref.shape[0]):
                mix = scores_ref[k:k + 1, :] / tally
                dense = dense + jnp.where(ids_ref[k:k + 1, :] == expert, mix, 0.0)
            lanes = wts.shape[2]
            dense = jnp.concatenate([dense, jnp.zeros((dense.shape[0], lanes), jnp.float32)], axis=1)
            mine_only = dense[:, :lanes]
            for k in range(1, count_tp):
                mine_only = jnp.where(tp == k, dense[:, k * rows:k * rows + lanes], mine_only)
            dense_ref[...] = mine_only
            wts[me] = mine_only
            for step in range(1, count_ep):
                mix_copy(step).start()
            for copy in mine_down:
                copy.wait()
            for q in reversed(range(QUARTERS)):
                over_x[DOWN[q]].start()
                to_near[DOWN[q]].start()
            for copy in mine:
                copy.wait()
            for i in (GATE, UP, UP_END):
                in_near[i].wait_recv()
            gate_up(0, 1, chip)
        if g == 5:
            gate_up(1, 2, chip)
        if g == 6:
            rin[none] = jnp.zeros(rin.shape[1:], rin.dtype)
            squares[...] = jnp.zeros_like(squares)
        if g == 7:
            gate_up(2, 3, chip)
            pass_on(GATE)
        if g == 8:
            for step in range(1, count_ep):
                mix_wait(step)
            for block in range(count_ep):
                turned = jnp.transpose(wts[block])
                lane = lax.broadcasted_iota(jnp.int32, turned.shape, 1)
                column = jnp.sum(jnp.where(lane == me, turned, 0.0), axis=1, keepdims=True)
                wcol[block] = jnp.broadcast_to(column[:rows], (rows, 128))
        if g == 9:
            gate_up(3, 4, chip)
        if g == 10:
            pass_on(UP)
        if g == 11:
            gate_up(4, 5, chip)
        if g == 12:
            pass_on(UP_END)
            for i in (GATE, UP, UP_END):
                in_onward[i].wait_recv()
            gate_up(3, 4, other_chip)
            gate_up(2, 3, other_chip)
        if g < BACK_START:
            continue
        r = g - BACK_START
        if r == 0:
            pass_on(DOWN[3])
            ready(3)
            back_slot(PAIR, 0)
            gate_up(5, 6, everyone)
            back_slot(INW, 0)
            back_slot(OUTW, 0)
            continue
        if r == 1:
            gate_up(6, 7, everyone)
            back_slot(PAIR, 1)
            pass_on(DOWN[2])
            ready(2)
            back_slot(INW, 1)
            back_slot(OUTW, 1)
            gate_up(4, 5, other_chip)
            continue
        if r == 4:
            ready(1)
        if r == 5:
            ready(0)
        if r < BACK:
            for link in links_back:
                back_slot(link, r)
        if r == 2:
            gate_up(0, 2, other_chip)
            pass_on(DOWN[1])
        if r == 3:
            gate_up(7, 8, everyone)
        if r == 4:
            pass_on(DOWN[0])
        if r >= BACK - 2:
            finish(BACK + 1 - r)

    mean = jnp.sum(squares[...], axis=1, keepdims=True) / width
    scale = lax.rsqrt(mean + epsilon)
    scales[tp, :, :rows] = jnp.transpose(jnp.broadcast_to(scale, squares.shape))[:scales.shape[1], :]

    def scale_copy(step):
        target = lax.rem(tp + step, count_tp)
        return remote(scales.at[tp], scales.at[tp], s_send.at[step - 1], s_recv.at[step - 1], me, target)

    def scale_wait(step):
        here = scales.at[lax.rem(tp + count_tp - step, count_tp)]
        remote(here, here, s_send.at[step - 1], s_recv.at[step - 1], me, tp).wait_recv()

    for step in range(1, count_tp):
        scale_copy(step).start()

    def result(source):
        return pltpu.make_async_copy(stage.at[source], out_ref.at[source], local_sem.at[source])

    for step in range(count_tp):
        source = lax.rem(tp + count_tp - step, count_tp)
        if step == 0:
            for q in range(QUARTERS):
                landed[tp, q] = fin[q, tp]
            column = scale
        else:
            scale_wait(step)
            column = jnp.transpose(scales[source])[:rows, :1]
            for q in range(QUARTERS):
                final_wait(q, step)
        for q in range(QUARTERS):
            at_columns = slice(q * sub, (q + 1) * sub)
            mixed = landed[source, q].astype(jnp.float32) * column * out_gain_ref[:, at_columns]
            stage[source, :, at_columns] = mixed.astype(jnp.bfloat16)
        result(source).start()

    for link in (INW, OUTW, PAIR):
        for s in range(SLOTS):
            for_kinds(at(SENDS, link, s), lambda a, b: row_copy(link, s, place(a, b)).wait_send())
        for s in range(BACK):
            for_kinds(at(BACK_SENDS, link, s), lambda a, b: back_copy(link, s).wait_send())
    for copies in (over_x, to_near, onward):
        for copy in copies:
            copy.wait_send()
    for step in range(1, count_ep):
        mix_copy(step).wait_send()
    for step in range(1, count_tp):
        scale_copy(step).wait_send()
        for q in range(QUARTERS):
            final_copy(q, step).wait_send()
    for source in range(count_tp):
        result(source).wait()


def fused(tokens, in_gain, route_ids, route_scores, gate_weight, up_weight, down_weight, out_gain):
    count_ep, count_tp = lax.axis_size("ep"), lax.axis_size("tp")
    experts = count_ep * gate_weight.shape[0]
    tok_count, width = tokens.shape
    rows = tok_count // count_tp
    part = gate_weight.shape[2]
    quarter = width // QUARTERS
    lanes = -(-rows // 128) * 128
    bf16, f32 = jnp.bfloat16, jnp.float32
    dma = pltpu.SemaphoreType.DMA
    any_space = pl.BlockSpec(memory_space=pltpu.HBM)
    weights = 3 + QUARTERS
    sub = width // count_tp // QUARTERS
    out = pl.pallas_call(
        fused_kernel,
        name="experts",
        out_shape=jax.ShapeDtypeStruct((count_tp, rows, width // count_tp), bf16),
        in_specs=[any_space] * 8,
        out_specs=any_space,
        scratch_shapes=[
            pltpu.VMEM((1, width), f32),
            pltpu.VMEM(route_ids.T.shape, route_ids.dtype),
            pltpu.VMEM(route_scores.T.shape, f32),
            pltpu.VMEM((1, width // count_tp), f32),
            pltpu.VMEM((rows, width), bf16),
            pltpu.VMEM((count_ep, rows, width), bf16),
            pltpu.VMEM((count_tp, width, part), bf16),
            pltpu.VMEM((count_tp, width, part), bf16),
            pltpu.VMEM((QUARTERS, count_tp, part, quarter), bf16),
            pltpu.VMEM((count_ep, rows, part * count_tp), bf16),
            pltpu.VMEM((3 * BACK + 1, rows, quarter), bf16),
            pltpu.VMEM((3 * BACK, rows, quarter), bf16),
            pltpu.VMEM((QUARTERS, count_tp, rows, sub), bf16),
            pltpu.VMEM((count_tp, QUARTERS, rows, sub), bf16),
            pltpu.VMEM((count_tp, rows, width // count_tp), bf16),
            pltpu.VMEM((rows, 128), f32),
            pltpu.VMEM((count_tp, 8, lanes), f32),
            pltpu.VMEM((experts, lanes), f32),
            pltpu.VMEM((count_ep, experts, lanes), f32),
            pltpu.VMEM((count_ep, rows, 128), f32),
            dma((3 + QUARTERS * count_tp,)),
            dma((4,)),
            dma((3, weights)),
            dma((3, weights)),
            dma((count_ep - 1,)),
            dma((count_ep - 1,)),
            dma((3, SLOTS)),
            dma((3, SLOTS)),
            dma((3, BACK)),
            dma((3, BACK)),
            dma((QUARTERS, count_tp - 1)),
            dma((QUARTERS, count_tp - 1)),
            dma((count_tp - 1,)),
            dma((count_tp - 1,)),
        ],
        compiler_params=pltpu.CompilerParams(
            collective_id=0, has_side_effects=True, vmem_limit_bytes=63 * 2**20
        ),
    )(
        tokens, in_gain.reshape(1, width), route_ids.T, route_scores.T, out_gain.reshape(1, -1),
        gate_weight[0], up_weight[0], down_weight[0],
    )
    return out.reshape(tok_count, width // count_tp)


def solution(mesh):
    in_specs = (
        P("ep", None),
        P(),
        P("ep", None),
        P("ep", None),
        P("ep", None, "tp"),
        P("ep", None, "tp"),
        P("ep", "tp", None),
        P("tp"),
    )
    out_specs = P("ep", "tp")
    small = mesh.shape["ep"] == 2 * LINE and mesh.shape["tp"] == QUARTERS
    return jax.shard_map(
        fused if small else per_device, mesh=mesh, in_specs=in_specs, out_specs=out_specs, check_vma=False
    )
```
